32 devices in a mesh: sp: 8 (over z, x), tp: 4 (over y, core).
Axes of the slice: x: 2, y: 2, z: 4, core: 2. Of those that a mesh axis runs over, the one named last changes fastest.
Arguments:
- stratum_source_matrix: bfloat16 [1024, 2048], P('sp'), may hold values from -70 to 70
- acceptance_query: bfloat16 [2, 1024, 1024], P(None, 'sp', 'tp'), may hold values from -6 to 6
- cluster_lookup_matrix: bfloat16 [2, 1024, 1024], P(None, 'sp', 'tp'), may hold values from -6 to 6
- cluster_payload_matrix: bfloat16 [2, 1024, 1024], P(None, 'sp', 'tp'), may hold values from -6 to 6
- fading_logit: bfloat16 [2, 1024, 1024], P(None, 'sp', 'tp'), may hold values from -17 to 2
- adaptation_speed_logit: bfloat16 [2, 1024, 1024], P(None, 'sp', 'tp'), may hold values from -14 to 5
- additional_fading_exponent: float32 [2, 1024, 1024], P(None, 'sp', 'tp'), may hold values from -0.7 to 0
- result_switch_pair: bfloat16 [2, 1024, 1024], P(None, 'sp', 'tp'), may hold values from -6 to 6
- attender_scaling_factor: float32 [2, 1024], P(None, 'tp'), may hold values from 0.1 to 1.9
- present_item_factor: float32 [2, 1024], P(None, 'tp'), may hold values from -0.9 to 0.9
- final_mapping_matrix: bfloat16 [2, 1024, 2048], P(None, 'tp'), may hold values from -0.125 to 0.125
- perceptron_scaling_factor: float32 [2048], replicated, may hold values from 0.1 to 1.9
- switching_matrix: bfloat16 [2048, 5632], P('sp', 'tp'), may hold values from -0.125 to 0.125
- widening_matrix: bfloat16 [2048, 5632], P('sp', 'tp'), may hold values from -0.125 to 0.125
- shrinking_matrix: bfloat16 [5632, 2048], P('tp', 'sp'), may hold values from -0.078125 to 0.078125
Outputs:
- layer_out: bfloat16 [1024, 2048], P('sp', 'tp')
The draws below stay inside these ranges and needn't reach their ends.
All inputs are finite; a program needn't handle non-finite values.
Results may differ from the reference program's by a relative error of at most 0.014.
Values may be sent and summed in bfloat16 or wider, within the bound.
A program may use at most 128 MiB of HBM per device.

```python
import math
import jax
import jax.numpy as jnp
from jax import lax

D = 2048
FF = 5632
CLUSTER_FEATURES = 1024
DS = 64
DL = 128
TOK_DEV = 128
SEQUENCE_TOKENS = 1024
N_TP = 4


def fast_heads(key):
    fast_share = 0.5
    small_heads = jax.random.uniform(jax.random.fold_in(key, 101), (CLUSTER_FEATURES // DS,)) < fast_share
    large_heads = jax.random.uniform(jax.random.fold_in(key, 102), (CLUSTER_FEATURES // DL,)) < fast_share
    return jnp.stack([jnp.repeat(small_heads, DS), jnp.repeat(large_heads, DL)])


def rough_entries(key):
    return jnp.clip(jax.random.normal(key, (2, SEQUENCE_TOKENS, CLUSTER_FEATURES)), -4.0, 4.0)


def draw_fading_logit(key, part):
    fast_mask = fast_heads(key)
    level = jnp.where(fast_mask, -3.5, -12.0)
    jitter = rough_entries(jax.random.fold_in(key, 201))
    block_shift = jax.random.uniform(jax.random.fold_in(key, 202), (2, SEQUENCE_TOKENS // TOK_DEV, 1), minval=-0.7, maxval=0.7)
    block_shift = jnp.repeat(block_shift, TOK_DEV, axis=1)
    return (level[:, None, :] + jitter + block_shift).astype(jnp.bfloat16)


def draw_adaptation_speed_logit(key, part):
    fast_mask = fast_heads(key)
    slow_small = math.log(0.4 * DS / SEQUENCE_TOKENS)
    slow_large = math.log(0.4 * DL / SEQUENCE_TOKENS)
    slow_level = jnp.stack([jnp.full((CLUSTER_FEATURES,), slow_small, jnp.float32), jnp.full((CLUSTER_FEATURES,), slow_large, jnp.float32)])
    level = jnp.where(fast_mask, 0.0, slow_level)
    jitter = rough_entries(jax.random.fold_in(key, 301))
    return (level[:, None, :] + jitter).astype(jnp.float32).astype(jnp.bfloat16)


def draw_additional_fading_exponent(key, part):
    extra_decay_rows = jax.random.randint(jax.random.fold_in(key, 401), (2, 3), 0, SEQUENCE_TOKENS)
    sequence_positions = jnp.arange(SEQUENCE_TOKENS)
    corrected_state = jnp.any(sequence_positions[None, :, None] == extra_decay_rows[:, None, :], axis=-1)
    extra_decay_depth = jax.random.uniform(jax.random.fold_in(key, 402), (2, SEQUENCE_TOKENS, CLUSTER_FEATURES), minval=math.log(0.5), maxval=math.log(0.8))
    return jnp.where(corrected_state[:, :, None], extra_decay_depth, 0.0).astype(jnp.float32)


def draw_stratum_source_matrix(key, part):
    spread = jnp.arange(D).astype(jnp.float32) / D
    column_scale = 0.5 * 3.0 ** spread * jnp.exp(jax.random.uniform(jax.random.fold_in(key, 501), (D,), minval=-0.6, maxval=0.6))
    row_scale = jnp.exp(jax.random.uniform(jax.random.fold_in(key, 502), (SEQUENCE_TOKENS, 1), minval=math.log(0.4), maxval=math.log(4.0)))
    entries = jnp.clip(jax.random.normal(jax.random.fold_in(key, 503), (SEQUENCE_TOKENS, D)), -6.0, 6.0)
    return (entries * row_scale * column_scale).astype(jnp.float32).astype(jnp.bfloat16)


def levels(own_key, extent, shards, smallest, top_value):
    factor_of = 1.0
    for axis_at, shards_of in shards:
        steps = jax.random.uniform(jax.random.fold_in(jax.random.fold_in(own_key, 6), axis_at), (shards_of,), jnp.float32, smallest / len(shards), top_value / len(shards))
        factor_of = factor_of * jnp.repeat(jnp.exp(steps), extent[axis_at] // shards_of).reshape((-1,) + (1,) * (len(extent) - 1 - axis_at))
    return factor_of


def scatter_about(own_key, dims, width, bound, shards=(), kind=jnp.bfloat16):
    loudness = levels(own_key, dims, shards, -0.22, 0.18) if shards else 1.0
    array = jax.random.normal(own_key, dims, jnp.float32) * width * loudness
    return jnp.minimum(jnp.maximum(array, -bound), bound).astype(kind)


def setup_inputs(seed: int = 0) -> dict:
    arg_keys = jax.random.split(jax.random.key(seed), 16)
    return {
        "stratum_source_matrix": draw_stratum_source_matrix(jax.random.fold_in(arg_keys[15], 71), 0),
        "acceptance_query": scatter_about(arg_keys[1], (2, SEQUENCE_TOKENS, CLUSTER_FEATURES), 1.0, 6.0, ((1, 8), (2, 4))),
        "cluster_lookup_matrix": scatter_about(arg_keys[2], (2, SEQUENCE_TOKENS, CLUSTER_FEATURES), 1.0, 6.0, ((1, 8), (2, 4))),
        "cluster_payload_matrix": scatter_about(arg_keys[3], (2, SEQUENCE_TOKENS, CLUSTER_FEATURES), 1.0, 6.0, ((1, 8), (2, 4))),
        "fading_logit": draw_fading_logit(jax.random.fold_in(arg_keys[15], 71), 0),
        "adaptation_speed_logit": draw_adaptation_speed_logit(jax.random.fold_in(arg_keys[15], 71), 0),
        "additional_fading_exponent": draw_additional_fading_exponent(jax.random.fold_in(arg_keys[15], 71), 0),
        "result_switch_pair": scatter_about(arg_keys[7], (2, SEQUENCE_TOKENS, CLUSTER_FEATURES), 1.0, 6.0, ((1, 8), (2, 4))),
        "attender_scaling_factor": jnp.clip(1.0 + 0.18 * jax.random.normal(arg_keys[8], (2, CLUSTER_FEATURES), jnp.float32), 0.1, 1.9),
        "present_item_factor": scatter_about(arg_keys[9], (2, CLUSTER_FEATURES), 0.15, 0.9, ((1, 4),), jnp.float32),
        "final_mapping_matrix": scatter_about(arg_keys[10], (2, CLUSTER_FEATURES, D), (2 * CLUSTER_FEATURES) ** -0.5, 0.125, ((1, 4),)),
        "perceptron_scaling_factor": jnp.clip(1.0 + 0.18 * jax.random.normal(arg_keys[11], (D,), jnp.float32), 0.1, 1.9),
        "switching_matrix": scatter_about(arg_keys[12], (D, FF), D ** -0.5, 0.125, ((0, 8), (1, 4))),
        "widening_matrix": scatter_about(arg_keys[13], (D, FF), D ** -0.5, 0.125, ((0, 8), (1, 4))),
        "shrinking_matrix": scatter_about(arg_keys[14], (FF, D), FF ** -0.5, 0.078125, ((0, 4), (1, 8))),
    }


highest = lax.Precision.HIGHEST
norm_epsilon = 1e-06
head_epsilon = 0.00064
key_epsilon = 1e-06

def per_head_terms(acceptance_query, cluster_lookup_matrix, cluster_payload_matrix, fading_logit, adaptation_speed_logit, additional_fading_exponent, attender_feature_count):
    row_count, channels = acceptance_query.shape
    lattice_layout = (row_count, channels // attender_feature_count, attender_feature_count)
    acceptance_lines = acceptance_query.astype(jnp.float32).reshape(lattice_layout)
    mapped_lookups = cluster_lookup_matrix.astype(jnp.float32).reshape(lattice_layout)
    mapped_payloads = cluster_payload_matrix.astype(jnp.float32).reshape(lattice_layout)
    learning_rate_logarithm = -jax.nn.softplus(-fading_logit.astype(jnp.float32)) - 0.5
    decay_logarithm = (additional_fading_exponent - jnp.exp(learning_rate_logarithm)).reshape(lattice_layout)
    learn_rate = jax.nn.sigmoid(adaptation_speed_logit.astype(jnp.float32)).reshape(lattice_layout)
    removal = mapped_lookups * lax.rsqrt(lax.optimization_barrier(jnp.sum(mapped_lookups * mapped_lookups, axis=-1, keepdims=True)) + key_epsilon)
    return (acceptance_lines, mapped_lookups, mapped_payloads, decay_logarithm, -removal, learn_rate * removal)

def entire_cluster(raw_retrieval, acceptance_lines, mapped_lookups, mapped_payloads, scaling_array, diagonal_reward_array, switch_amounts):
    row_count, attender_count, attender_feature_count = raw_retrieval.shape
    row_mean = lax.optimization_barrier(jnp.mean(raw_retrieval, axis=-1, keepdims=True))
    centered = raw_retrieval - row_mean
    variance = lax.optimization_barrier(jnp.mean(centered * centered, axis=-1, keepdims=True))
    normed = centered * lax.rsqrt(variance + head_epsilon) * scaling_array.reshape(attender_count, attender_feature_count)
    diagonal_item_contribution = lax.optimization_barrier(jnp.sum(acceptance_lines * mapped_lookups * diagonal_reward_array.reshape(attender_count, attender_feature_count), axis=-1, keepdims=True)) * mapped_payloads
    joined = (normed + diagonal_item_contribution).reshape(row_count, attender_count * attender_feature_count)
    return (joined * switch_amounts.astype(jnp.float32)).astype(jnp.bfloat16)

def advance_one(memory, acceptance_lines, mapped_lookups, mapped_payloads, decay_logarithm, remove_left, remove_right):
    removed = jnp.einsum('hij,hj->hi', memory, remove_left, precision=highest)
    memory = memory * jnp.exp(decay_logarithm)[:, None, :] + removed[:, :, None] * remove_right[:, None, :] + mapped_payloads[:, :, None] * mapped_lookups[:, None, :]
    return (memory, jnp.einsum('hij,hj->hi', memory, acceptance_lines, precision=highest))

def recurrence(terms_small, terms_large):

    def advance(memories, inputs):
        memory_small, read_small = advance_one(memories[0], *inputs[0])
        memory_large, read_large = advance_one(memories[1], *inputs[1])
        return ((memory_small, memory_large), (read_small, read_large))
    initial = tuple((jnp.zeros((aggregated_contributions[0].shape[1], aggregated_contributions[0].shape[2], aggregated_contributions[0].shape[2]), jnp.float32) for aggregated_contributions in (terms_small, terms_large)))
    final_memories, retrieved_result_lines = lax.scan(advance, initial, (terms_small, terms_large))
    return retrieved_result_lines

def reference(stratum_source_matrix, acceptance_query, cluster_lookup_matrix, cluster_payload_matrix, fading_logit, adaptation_speed_logit, additional_fading_exponent, result_switch_pair, attender_scaling_factor, present_item_factor, final_mapping_matrix, perceptron_scaling_factor, switching_matrix, widening_matrix, shrinking_matrix):
    group_widths = (DS, DL)
    aggregated_contributions = [per_head_terms(acceptance_query[cluster_ordinal], cluster_lookup_matrix[cluster_ordinal], cluster_payload_matrix[cluster_ordinal], fading_logit[cluster_ordinal], adaptation_speed_logit[cluster_ordinal], additional_fading_exponent[cluster_ordinal], group_widths[cluster_ordinal]) for cluster_ordinal in range(2)]
    retrieved_result_lines = recurrence(tuple(aggregated_contributions[0]), tuple(aggregated_contributions[1]))
    blended_result = [entire_cluster(retrieved_result_lines[cluster_ordinal], aggregated_contributions[cluster_ordinal][0], aggregated_contributions[cluster_ordinal][1], aggregated_contributions[cluster_ordinal][2], attender_scaling_factor[cluster_ordinal], present_item_factor[cluster_ordinal], result_switch_pair[cluster_ordinal]) for cluster_ordinal in range(2)]
    slice_width = CLUSTER_FEATURES // N_TP
    branch = jnp.zeros((SEQUENCE_TOKENS, D), jnp.float32)
    for slice_index in range(N_TP):
        lower = slice_index * slice_width
        upper = lower + slice_width
        partial_value = jnp.dot(blended_result[0][:, lower:upper], final_mapping_matrix[0, lower:upper], preferred_element_type=jnp.float32) + jnp.dot(blended_result[1][:, lower:upper], final_mapping_matrix[1, lower:upper], preferred_element_type=jnp.float32)
        branch = branch + lax.optimization_barrier(partial_value.astype(jnp.bfloat16)).astype(jnp.float32)
    hidden_state = (stratum_source_matrix.astype(jnp.float32) + branch).astype(jnp.bfloat16)
    state_float = hidden_state.astype(jnp.float32)
    mean_square = lax.optimization_barrier(jnp.mean(state_float * state_float, axis=1, keepdims=True))
    normed = (state_float * lax.rsqrt(mean_square + norm_epsilon) * perceptron_scaling_factor).astype(jnp.bfloat16)
    gate_pre = jnp.dot(normed, switching_matrix, preferred_element_type=jnp.float32)
    up_pre = jnp.dot(normed, widening_matrix, preferred_element_type=jnp.float32)
    activated = (jax.nn.silu(gate_pre) * up_pre).astype(jnp.bfloat16)
    hidden_width = FF // N_TP
    mixer = jnp.zeros((SEQUENCE_TOKENS, D), jnp.float32)
    for slice_index in range(N_TP):
        lower = slice_index * hidden_width
        upper = lower + hidden_width
        partial_value = jnp.dot(activated[:, lower:upper], shrinking_matrix[lower:upper], preferred_element_type=jnp.float32)
        mixer = mixer + lax.optimization_barrier(partial_value.astype(jnp.bfloat16)).astype(jnp.float32)
    return (state_float + mixer).astype(jnp.bfloat16)
```

```python
import functools

import jax
import jax.numpy as jnp
from jax import lax
from jax.experimental import pallas as pl
from jax.experimental.pallas import tpu as pltpu
from jax.sharding import PartitionSpec as P

DS = 64
DL = 128
LANES = 128
MESH = pl.DeviceIdType.MESH

norm_epsilon = 1e-06
head_epsilon = 0.00064
key_epsilon = 1e-06


NN = (((1,), (0,)), ((), ()))
NT = (((1,), (1,)), ((), ()))


def split(x, count=2):
    if x.dtype == jnp.bfloat16:
        return [x]
    parts = []
    for _ in range(count - 1):
        high = x.astype(jnp.bfloat16)
        parts.append(high)
        x = x - high.astype(jnp.float32)
    return parts + [x.astype(jnp.bfloat16)]


def product(a, b, dims, count=2):
    total = None
    for i, p in enumerate(split(a, count)):
        for j, r in enumerate(split(b, count)):
            if i + j < count:
                term = lax.dot_general(p, r, dims, preferred_element_type=jnp.float32)
                total = term if total is None else total + term
    return total


def mm(a, b, count=2):
    return product(a, b, NN, count)


def mm_nt(a, b):
    return product(a, b, NT)


def sigmoid(x):
    return 1.0 / (1.0 + jnp.exp(-x))


def same_head(width):
    i = lax.broadcasted_iota(jnp.int32, (LANES, LANES), 0) // width
    j = lax.broadcasted_iota(jnp.int32, (LANES, LANES), 1) // width
    return (i == j).astype(jnp.float32).astype(jnp.bfloat16)


def unit_inverse(strict_part, rows, cols):
    size = strict_part.shape[0]
    inverse = (rows == cols).astype(jnp.float32)
    half = 1
    while half < size:
        off = (rows // (2 * half) == cols // (2 * half)) & (rows // half != cols // half)
        part = jnp.where(off, strict_part, 0.0)
        if half == 1:
            inverse = inverse + part
        else:
            inverse = inverse + mm(mm(inverse, part), inverse)
        half *= 2
    return inverse


def local_unit(width, q, k, v, fade, speed, extra):
    T = q.shape[0]
    ones = same_head(width)
    log_decay = extra - jnp.exp(jnp.float32(-0.5)) * sigmoid(fade)
    removal = k * lax.rsqrt(mm(k * k, ones) + key_epsilon)
    left = -removal
    right = sigmoid(speed) * removal
    rows = lax.broadcasted_iota(jnp.int32, (T, T), 0)
    cols = lax.broadcasted_iota(jnp.int32, (T, T), 1)
    inclusive = rows >= cols
    strict = rows > cols
    cumulative = mm(inclusive.astype(jnp.float32).astype(jnp.bfloat16), log_decay, 3)
    middle = cumulative[T // 2 : T // 2 + 1, :]
    final = cumulative[T - 1 : T, :]
    forward = jnp.exp(cumulative - middle)
    backward = jnp.exp(middle - cumulative)
    tail = jnp.exp(final - cumulative)
    queries = jnp.concatenate([left * jnp.exp(-log_decay) * forward, q * forward], axis=0)
    sources = jnp.concatenate([right * backward, k * backward], axis=0)
    start_target = left * jnp.exp(cumulative - log_decay)
    right_tail = right * tail
    key_tail = k * tail
    eye = lax.broadcasted_iota(jnp.int32, (LANES, LANES), 0) == lax.broadcasted_iota(
        jnp.int32, (LANES, LANES), 1
    )
    transit = jnp.where(eye, jnp.exp(final), 0.0)
    start_read = q * jnp.exp(cumulative)
    added = jnp.zeros((LANES, LANES), jnp.float32)
    local_out = jnp.zeros((T, LANES), jnp.float32)
    lane = lax.broadcasted_iota(jnp.int32, (1, LANES), 1) // width
    for head in range(LANES // width):
        only = lane == head
        pick = (lambda a: a) if width == LANES else (lambda a: jnp.where(only, a, 0.0))
        pairs = mm_nt(pick(queries), sources)
        remove_remove = jnp.where(strict, pairs[:T, :T], 0.0)
        remove_key = jnp.where(strict, pairs[:T, T:], 0.0)
        read_remove = jnp.where(inclusive, pairs[T:, :T], 0.0)
        read_key = jnp.where(inclusive, pairs[T:, T:], 0.0)
        inverse = unit_inverse(remove_remove, rows, cols)
        value = pick(v)
        carried = mm(inverse, mm(remove_key, value))
        start = mm(inverse, pick(start_target))
        local_out = local_out + mm(read_remove, carried) + mm(read_key, value)
        start_read = start_read + mm(read_remove, start)
        head_right = pick(right_tail)
        transit = transit + mm(start.T, head_right)
        added = added + mm(carried.T, head_right) + mm(value.T, pick(key_tail))
    return local_out, start_read, transit, added


def finish_unit(width, read, q, k, v, gain, own, gate):
    ones = same_head(width)
    mean = mm(read, ones) / width
    centered = read - mean
    variance = mm(centered * centered, ones) / width
    normed = centered * lax.rsqrt(variance + head_epsilon) * gain
    diagonal = mm(q * k * own, ones) * v
    return ((normed + diagonal) * gate).astype(jnp.bfloat16)


def members_of(n_sp):
    best = 1
    for count in range(1, n_sp + 1):
        if n_sp % count == 0 and count * count <= 2 * n_sp:
            best = count
    return best


def layer_kernel(
    n_sp, n_tp, widths, q_ref, k_ref, v_ref, f_ref, a_ref, e_ref, g_ref, gain_ref, own_ref,
    residual_ref, scale_ref, project_hbm, gate_hbm, up_hbm, down_hbm,
    out_ref,
    local_ref, read_ref, near, total_move, total_add, chain_in, chain_out, mixed_ref, project,
    wide, tall, term_send, term_got, hidden, active, summed,
    low_send, low_got, high_send, high_got, line_send, line_got,
    project_sem, keep_sem, out_sem, in_sem, pass_out, pass_in,
    near_out, near_in, chain_sem_out, chain_sem_in, term_out, term_in,
    row_out, row_in, up_out, up_in, side_out, side_in,
    low_out, low_in, high_out, high_in, line_out, line_in,
):
    F = members_of(n_sp)
    T = n_sp // F
    LO = 2 if n_tp % 2 == 0 else 1
    HI = n_tp // LO
    me = lax.axis_index("sp")
    t = lax.axis_index("tp")
    m, g = me // T, me % T
    hi, lo = t // LO, t % LO
    tokens = q_ref.shape[1]
    rows = gate_hbm.shape[0]
    depth = hidden.shape[1]
    own_cols = depth // n_tp
    down_cols = down_hbm.shape[1]
    base, extra = divmod(gate_hbm.shape[1] // LANES, F)
    parts = 2 if extra else 1

    def member(d):
        return lax.rem(m + d + F, F)

    def other(e):
        return lax.rem(g + e + T, T)

    def cell(h, l):
        return lax.rem(hi + h + HI, HI) * LO + lax.rem(lo + l + LO, LO)

    def remote(src, dst, send, recv, sp, tp):
        return pltpu.make_async_remote_copy(
            src_ref=src, dst_ref=dst, send_sem=send, recv_sem=recv,
            device_id=(sp, tp), device_id_type=MESH,
        )

    barrier = pltpu.get_barrier_semaphore()

    def greet(sp, tp):
        pl.semaphore_signal(barrier, inc=1, device_id=(sp, tp), device_id_type=MESH)

    for d in range(1, F):
        greet(member(d) * T + g, t)
    for e in range(1, T):
        greet(m * T + other(e), t)
    for d in range(1, n_tp):
        greet(me, lax.rem(t + d, n_tp))
    project_copy = pltpu.make_async_copy(project_hbm, project, project_sem)
    project_copy.start()
    pl.semaphore_wait(barrier, F + T + n_tp - 3)

    def source(w, part, dest):
        tile = dest * base + jnp.minimum(dest, extra) + (base if part else 0)
        at = pl.ds(pl.multiple_of(tile * LANES, LANES), LANES if part else base * LANES)
        return down_hbm.at[at, :] if w == 2 else (gate_hbm, up_hbm)[w].at[:, at]

    def landing(w, part, s):
        at = pl.ds(base * LANES if part else 0, LANES if part else base * LANES)
        if w == 2:
            return tall.at[s, at, :]
        return wide.at[w, pl.ds(pl.multiple_of(s * rows, rows), rows), at]

    def guarded(part, dest, action):
        if part:
            pl.when(dest < extra)(action)
        else:
            action()

    def give(w, part, d):
        dest = member(d)
        return remote(
            source(w, part, dest), landing(w, part, me), out_sem.at[w, part, d],
            in_sem.at[w, part, d], dest * T + g, t,
        )

    def take(w, part, d):
        return remote(
            source(w, part, m), landing(w, part, member(-d) * T + g), out_sem.at[w, part, d],
            in_sem.at[w, part, d], me, t,
        )

    def hand(w, part, d, e):
        s = member(-d) * T + g
        src = source(w, part, m) if d == 0 else landing(w, part, s)
        return remote(
            src, landing(w, part, s), pass_out.at[w, part, d, e], pass_in.at[w, part, d, e],
            m * T + other(e), t,
        )

    def accept(w, part, d, e):
        s = member(-d) * T + other(-e)
        return remote(
            source(w, part, m), landing(w, part, s), pass_out.at[w, part, d, e],
            pass_in.at[w, part, d, e], me, t,
        )

    def keep(w, part):
        return pltpu.make_async_copy(
            source(w, part, m), landing(w, part, me), keep_sem.at[w, part]
        )

    def open_weight(w):
        for part in range(parts):

            def begin():
                keep(w, part).start()
                for e in range(1, T):
                    hand(w, part, 0, e).start()

            guarded(part, m, begin)

    def send_weight(w, upward):
        for d in range(F - 1, 0, -1):
            for part in range(parts):
                dest = member(d)
                chosen = dest > m if upward else dest < m
                if part:
                    chosen = chosen & (dest < extra)
                pl.when(chosen)(lambda: give(w, part, d).start())

    def relay_weight(w):
        for d in range(1, F):
            for part in range(parts):

                def pass_on():
                    take(w, part, d).wait_recv()
                    for e in range(1, T):
                        hand(w, part, d, e).start()

                guarded(part, m, pass_on)

    def arrived_weight(w):
        for part in range(parts):

            def settle():
                keep(w, part).wait()
                for d in range(F):
                    for e in range(1, T):
                        accept(w, part, d, e).wait_recv()

            guarded(part, m, settle)

    open_weight(0)
    send_weight(0, True)
    send_weight(0, False)
    if extra:

        @pl.when(m >= extra)
        def _():
            tall[:, base * LANES :, :] = jnp.zeros(
                (n_sp, LANES, down_cols), jnp.bfloat16
            )

    per_group = q_ref.shape[2] // LANES

    def load(ref, group, c):
        return ref[group, :, c * LANES : (c + 1) * LANES].astype(jnp.float32)

    units = [(group, c) for group in range(2) for c in range(per_group)]

    def near_copy(u, e):
        return remote(
            near.at[g, u], near.at[g, u], near_out.at[u, e], near_in.at[u, e],
            m * T + other(e), t,
        )

    def near_take(u, e):
        return remote(
            near.at[other(-e), u], near.at[other(-e), u], near_out.at[u, e],
            near_in.at[u, e], me, t,
        )

    for u, (group, c) in enumerate(units):
        local_out, start_read, transit, added = local_unit(
            widths[group],
            *(load(r, group, c) for r in (q_ref, k_ref, v_ref, f_ref, a_ref, e_ref)),
        )
        local_ref[u] = local_out
        read_ref[u] = start_read
        near[g, u, 0] = transit.astype(jnp.bfloat16)
        near[g, u, 1] = added.astype(jnp.bfloat16)
    for u in range(len(units)):
        for e in range(1, T):
            near_copy(u, e).start()

    @pl.when(m == 0)
    def _():
        chain_in[...] = jnp.zeros_like(chain_in)

    send_weight(1, False)
    open_weight(1)
    relay_weight(0)

    def chain_copy(u):
        return remote(
            chain_out.at[u], chain_in.at[u], chain_sem_out.at[u], chain_sem_in.at[u],
            member(1) * T + g, t,
        )

    for u in range(len(units)):
        for e in range(1, T):
            near_take(u, e).wait_recv()
        move, add = near[0, u, 0], near[0, u, 1].astype(jnp.float32)
        for other_g in range(1, T):
            step = near[other_g, u, 0]
            add = mm(add, step) + near[other_g, u, 1].astype(jnp.float32)
            move = mm(move, step).astype(jnp.bfloat16)
        total_move[u] = move
        total_add[u] = add
    for u in range(len(units)):

        @pl.when(m > 0)
        def _():
            chain_copy(u).wait_recv()

        following = mm(chain_in[u], total_move[u]) + total_add[u]
        chain_out[u] = following.astype(jnp.bfloat16)

        @pl.when(m < F - 1)
        def _():
            chain_copy(u).start()

    send_weight(1, True)

    def fold(other_g, states):
        return tuple(
            mm(s, near[other_g, u, 0]) + near[other_g, u, 1].astype(jnp.float32)
            for u, s in enumerate(states)
        )

    states = lax.fori_loop(
        0, g, fold, tuple(chain_in[u].astype(jnp.float32) for u in range(len(units)))
    )
    for u, (group, c) in enumerate(units):
        lanes = slice(c * LANES, (c + 1) * LANES)
        read = local_ref[u] + mm_nt(read_ref[u], states[u])
        mixed_ref[:, u * LANES : (u + 1) * LANES] = finish_unit(
            widths[group], read, load(q_ref, group, c), load(k_ref, group, c),
            load(v_ref, group, c), gain_ref[group : group + 1, lanes],
            own_ref[group : group + 1, lanes], load(g_ref, group, c),
        )

    project_copy.wait()
    mixed = mixed_ref[...]

    def columns(at):
        return pl.ds(pl.multiple_of(at * own_cols, own_cols), own_cols)

    def term(at):
        return jnp.dot(mixed, project[:, columns(at)], preferred_element_type=jnp.float32)

    def term_copy(d):
        return remote(
            term_send.at[d], term_got.at[d], term_out.at[d], term_in.at[d],
            me, lax.rem(t + d, n_tp),
        )

    for d in range(1, n_tp):
        term_send[d] = term(lax.rem(t + d, n_tp)).astype(jnp.bfloat16)
        term_copy(d).start()
    branch = term(t).astype(jnp.bfloat16).astype(jnp.float32)
    open_weight(2)
    send_weight(2, True)
    send_weight(2, False)
    relay_weight(1)
    for d in range(1, n_tp):
        term_copy(d).wait_recv()
        branch = branch + term_got[d].astype(jnp.float32)

    def positions(at):
        return pl.ds(pl.multiple_of(at * tokens, tokens), tokens)

    own_state = (residual_ref[:, columns(t)].astype(jnp.float32) + branch).astype(jnp.bfloat16)
    hidden[positions(m), columns(t)] = own_state

    def row_copy(d):
        block = hidden.at[positions(m), columns(t)]
        return remote(block, block, row_out.at[d], row_in.at[d], member(d) * T + g, t)

    def row_take(d):
        block = hidden.at[positions(member(-d)), columns(t)]
        return remote(block, block, row_out.at[d], row_in.at[d], me, t)

    def up_copy(d, h):
        block = hidden.at[positions(member(-d)), columns(t)]
        return remote(block, block, up_out.at[d, h], up_in.at[d, h], me, cell(h, 0))

    def up_take(d, h):
        block = hidden.at[positions(member(-d)), columns(cell(-h, 0))]
        return remote(block, block, up_out.at[d, h], up_in.at[d, h], me, t)

    def side_copy(d, h, l):
        block = hidden.at[positions(member(-d)), columns(cell(-h, 0))]
        return remote(block, block, side_out.at[d, h, l], side_in.at[d, h, l], me, cell(0, l))

    def side_take(d, h, l):
        block = hidden.at[positions(member(-d)), columns(cell(-h, -l))]
        return remote(block, block, side_out.at[d, h, l], side_in.at[d, h, l], me, t)

    for d in range(F - 1, 0, -1):
        row_copy(d).start()
    for d in range(F + 1):
        if d < F:
            if d:
                row_take(d).wait_recv()
            for h in range(1, HI):
                up_copy(d, h).start()
            for l in range(1, LO):
                side_copy(d, 0, l).start()
        if d:
            for h in range(1, HI):
                up_take(d - 1, h).wait_recv()
                for l in range(1, LO):
                    side_copy(d - 1, h, l).start()
    for d in range(F):
        for h in range(HI):
            for l in range(1, LO):
                side_take(d, h, l).wait_recv()

    arrived_weight(0)
    arrived_weight(1)
    width = wide.shape[2]
    have = (base + (m < extra).astype(jnp.int32)) * LANES if extra else width

    @pl.loop(0, F)
    def _(i):
        state = hidden[positions(i), :].astype(jnp.float32)
        power = jnp.sum(state * state, axis=1, keepdims=True) / depth
        normed = (state * lax.rsqrt(power + norm_epsilon) * scale_ref[...]).astype(jnp.bfloat16)
        gate_pre = jnp.dot(normed, wide[0], preferred_element_type=jnp.float32)
        up_pre = jnp.dot(normed, wide[1], preferred_element_type=jnp.float32)
        value = gate_pre / (1.0 + jnp.exp(-gate_pre)) * up_pre
        if extra:
            lane = lax.broadcasted_iota(jnp.int32, (1, width), 1)
            value = jnp.where(lane < have, value, 0.0)
        active[positions(i), :] = value.astype(jnp.bfloat16)

    relay_weight(2)
    arrived_weight(2)

    @pl.loop(0, F)
    def _(i):
        block = active[positions(i), :]
        for s in range(n_sp):
            summed[positions(i), s * down_cols : (s + 1) * down_cols] = jnp.dot(
                block, tall[s], preferred_element_type=jnp.float32
            )

    def low_copy(d, h, l):
        return remote(
            low_send.at[d, h, l], low_got.at[d, h, l], low_out.at[d, h, l],
            low_in.at[d, h, l], me, cell(0, l),
        )

    def high_copy(d, h):
        return remote(
            high_send.at[d, h], high_got.at[d, h], high_out.at[d, h], high_in.at[d, h],
            me, cell(h, 0),
        )

    def line_copy(d):
        return remote(
            line_send.at[d], line_got.at[d], line_out.at[d], line_in.at[d], member(d) * T + g, t
        )

    order = list(range(F - 1, 0, -1)) + [0]
    for d in order:
        for h in range(HI):
            for l in range(1, LO):
                low_send[d, h, l] = summed[positions(member(d)), columns(cell(h, l))].astype(
                    jnp.bfloat16
                )
                low_copy(d, h, l).start()

    def two_cores(d, h):
        value = summed[positions(member(d)), columns(cell(h, 0))]
        for l in range(1, LO):
            value = value + low_got[d, h, l].astype(jnp.float32)
        return value

    for d in order:
        for h in range(HI):
            for l in range(1, LO):
                low_copy(d, h, l).wait_recv()
        for h in range(1, HI):
            high_send[d, h] = two_cores(d, h).astype(jnp.bfloat16)
            high_copy(d, h).start()

    for d in order:
        value = two_cores(d, 0)
        for h in range(1, HI):
            high_copy(d, h).wait_recv()
            value = value + high_got[d, h].astype(jnp.float32)
        if d:
            line_send[d] = value.astype(jnp.bfloat16)
            line_copy(d).start()
    for d in range(1, F):
        line_copy(d).wait_recv()
        value = value + line_got[d].astype(jnp.float32)
    out_ref[...] = (
        hidden[positions(m), columns(t)].astype(jnp.float32) + value
    ).astype(jnp.bfloat16)

    for w in range(3):
        for part in range(parts):
            for d in range(1, F):
                guarded(part, member(d), lambda: give(w, part, d).wait_send())

            def passed():
                for d in range(F):
                    for e in range(1, T):
                        hand(w, part, d, e).wait_send()

            guarded(part, m, passed)
    for u in range(len(units)):
        for e in range(1, T):
            near_copy(u, e).wait_send()

    @pl.when(m < F - 1)
    def _():
        for u in range(len(units)):
            chain_copy(u).wait_send()

    for d in range(1, n_tp):
        term_copy(d).wait_send()
    for d in range(F):
        if d:
            row_copy(d).wait_send()
            line_copy(d).wait_send()
        for h in range(HI):
            if h:
                up_copy(d, h).wait_send()
                high_copy(d, h).wait_send()
            for l in range(1, LO):
                side_copy(d, h, l).wait_send()
                low_copy(d, h, l).wait_send()


def layer(n_sp, n_tp, q, k, v, f, a, e, g, gain, own, residual, scale, project, gate, up, down):
    tokens, channels = q.shape[1], q.shape[2]
    units = 2 * channels // LANES
    depth = residual.shape[1]
    cols = depth // n_tp
    F = members_of(n_sp)
    T = n_sp // F
    LO = 2 if n_tp % 2 == 0 else 1
    HI = n_tp // LO
    width = -(-(gate.shape[1] // LANES) // F) * LANES
    vmem = pl.BlockSpec(memory_space=pltpu.VMEM)
    hbm = pl.BlockSpec(memory_space=pl.ANY)
    bf16, f32 = jnp.bfloat16, jnp.float32
    sem = pltpu.SemaphoreType.DMA
    scratch = [
        pltpu.VMEM((units, tokens, LANES), f32),
        pltpu.VMEM((units, tokens, LANES), f32),
        pltpu.VMEM((T, units, 2, LANES, LANES), bf16),
        pltpu.VMEM((units, LANES, LANES), bf16),
        pltpu.VMEM((units, LANES, LANES), f32),
        pltpu.VMEM((units, LANES, LANES), bf16),
        pltpu.VMEM((units, LANES, LANES), bf16),
        pltpu.VMEM((tokens, units * LANES), bf16),
        pltpu.VMEM(project.shape, bf16),
        pltpu.VMEM((2, depth, width), bf16),
        pltpu.VMEM((n_sp, width, down.shape[1]), bf16),
        pltpu.VMEM((n_tp, tokens, cols), bf16),
        pltpu.VMEM((n_tp, tokens, cols), bf16),
        pltpu.VMEM((F * tokens, depth), bf16),
        pltpu.VMEM((F * tokens, width), bf16),
        pltpu.VMEM((F * tokens, depth), f32),
        pltpu.VMEM((F, HI, LO, tokens, cols), bf16),
        pltpu.VMEM((F, HI, LO, tokens, cols), bf16),
        pltpu.VMEM((F, HI, tokens, cols), bf16),
        pltpu.VMEM((F, HI, tokens, cols), bf16),
        pltpu.VMEM((F, tokens, cols), bf16),
        pltpu.VMEM((F, tokens, cols), bf16),
        sem, sem((3, 2)),
    ]
    for shape in (
        (3, 2, F), (3, 2, F, T), (units, T), (units,), (n_tp,), (F,), (F, HI), (F, HI, LO),
        (F, HI, LO), (F, HI), (F,),
    ):
        scratch += [sem(shape), sem(shape)]
    return pl.pallas_call(
        functools.partial(layer_kernel, n_sp, n_tp, (DS, DL)),
        out_shape=jax.ShapeDtypeStruct((tokens, cols), bf16),
        in_specs=[vmem] * 11 + [hbm] * 4,
        out_specs=vmem,
        scratch_shapes=scratch,
        compiler_params=pltpu.CompilerParams(
            collective_id=0, has_side_effects=True, vmem_limit_bytes=60 * 2**20
        ),
        name="layer",
    )(q, k, v, f, a, e, g, gain, own, residual, scale, project, gate, up, down)


def on_device(
    stratum_source_matrix,
    acceptance_query,
    cluster_lookup_matrix,
    cluster_payload_matrix,
    fading_logit,
    adaptation_speed_logit,
    additional_fading_exponent,
    result_switch_pair,
    attender_scaling_factor,
    present_item_factor,
    final_mapping_matrix,
    perceptron_scaling_factor,
    switching_matrix,
    widening_matrix,
    shrinking_matrix,
):
    return layer(
        lax.axis_size("sp"),
        lax.axis_size("tp"),
        acceptance_query,
        cluster_lookup_matrix,
        cluster_payload_matrix,
        fading_logit,
        adaptation_speed_logit,
        additional_fading_exponent,
        result_switch_pair,
        attender_scaling_factor,
        present_item_factor,
        stratum_source_matrix,
        perceptron_scaling_factor.reshape(1, -1),
        final_mapping_matrix.reshape(-1, final_mapping_matrix.shape[2]),
        switching_matrix,
        widening_matrix,
        shrinking_matrix,
    )


def solution(mesh):
    tokens = P(None, "sp", "tp")
    in_specs = (
        P("sp", None), tokens, tokens, tokens, tokens, tokens, tokens, tokens,
        P(None, "tp"), P(None, "tp"), P(None, "tp", None), P(),
        P("sp", "tp"), P("sp", "tp"), P("tp", "sp"),
    )
    return jax.shard_map(
        on_device, mesh=mesh, in_specs=in_specs, out_specs=P("sp", "tp"), check_vma=False
    )
```

```python
import functools

import jax
import jax.numpy as jnp
from jax import lax
from jax.experimental import pallas as pl
from jax.experimental.pallas import tpu as pltpu
from jax.sharding import PartitionSpec as P

DS = 64
DL = 128
LANES = 128
MESH = pl.DeviceIdType.MESH

norm_epsilon = 1e-06
head_epsilon = 0.00064
key_epsilon = 1e-06


NN = (((1,), (0,)), ((), ()))
NT = (((1,), (1,)), ((), ()))


def split(x, count=2):
    if x.dtype == jnp.bfloat16:
        return [x]
    parts = []
    for _ in range(count - 1):
        high = x.astype(jnp.bfloat16)
        parts.append(high)
        x = x - high.astype(jnp.float32)
    return parts + [x.astype(jnp.bfloat16)]


def product(a, b, dims, count=2):
    total = None
    for i, p in enumerate(split(a, count)):
        for j, r in enumerate(split(b, count)):
            if i + j < count:
                term = lax.dot_general(p, r, dims, preferred_element_type=jnp.float32)
                total = term if total is None else total + term
    return total


def mm(a, b, count=2):
    return product(a, b, NN, count)


def mm_nt(a, b):
    return product(a, b, NT)


def sigmoid(x):
    return 1.0 / (1.0 + jnp.exp(-x))


def same_head(width):
    i = lax.broadcasted_iota(jnp.int32, (LANES, LANES), 0) // width
    j = lax.broadcasted_iota(jnp.int32, (LANES, LANES), 1) // width
    return (i == j).astype(jnp.float32).astype(jnp.bfloat16)


def unit_inverse(strict_part, rows, cols):
    size = strict_part.shape[0]
    inverse = (rows == cols).astype(jnp.float32)
    half = 1
    while half < size:
        off = (rows // (2 * half) == cols // (2 * half)) & (rows // half != cols // half)
        part = jnp.where(off, strict_part, 0.0)
        if half == 1:
            inverse = inverse + part
        else:
            inverse = inverse + mm(mm(inverse, part), inverse)
        half *= 2
    return inverse


def local_unit(width, q, k, v, fade, speed, extra):
    T = q.shape[0]
    ones = same_head(width)
    log_decay = extra - jnp.exp(jnp.float32(-0.5)) * sigmoid(fade)
    removal = k * lax.rsqrt(mm(k * k, ones) + key_epsilon)
    left = -removal
    right = sigmoid(speed) * removal
    rows = lax.broadcasted_iota(jnp.int32, (T, T), 0)
    cols = lax.broadcasted_iota(jnp.int32, (T, T), 1)
    inclusive = rows >= cols
    strict = rows > cols
    cumulative = mm(inclusive.astype(jnp.float32).astype(jnp.bfloat16), log_decay, 3)
    middle = cumulative[T // 2 : T // 2 + 1, :]
    final = cumulative[T - 1 : T, :]
    forward = jnp.exp(cumulative - middle)
    backward = jnp.exp(middle - cumulative)
    tail = jnp.exp(final - cumulative)
    queries = jnp.concatenate([left * jnp.exp(-log_decay) * forward, q * forward], axis=0)
    sources = jnp.concatenate([right * backward, k * backward], axis=0)
    start_target = left * jnp.exp(cumulative - log_decay)
    right_tail = right * tail
    key_tail = k * tail
    eye = lax.broadcasted_iota(jnp.int32, (LANES, LANES), 0) == lax.broadcasted_iota(
        jnp.int32, (LANES, LANES), 1
    )
    transit = jnp.where(eye, jnp.exp(final), 0.0)
    start_read = q * jnp.exp(cumulative)
    added = jnp.zeros((LANES, LANES), jnp.float32)
    local_out = jnp.zeros((T, LANES), jnp.float32)
    lane = lax.broadcasted_iota(jnp.int32, (1, LANES), 1) // width
    for head in range(LANES // width):
        only = lane == head
        pick = (lambda a: a) if width == LANES else (lambda a: jnp.where(only, a, 0.0))
        pairs = mm_nt(pick(queries), sources)
        remove_remove = jnp.where(strict, pairs[:T, :T], 0.0)
        remove_key = jnp.where(strict, pairs[:T, T:], 0.0)
        read_remove = jnp.where(inclusive, pairs[T:, :T], 0.0)
        read_key = jnp.where(inclusive, pairs[T:, T:], 0.0)
        inverse = unit_inverse(remove_remove, rows, cols)
        value = pick(v)
        carried = mm(inverse, mm(remove_key, value))
        start = mm(inverse, pick(start_target))
        local_out = local_out + mm(read_remove, carried) + mm(read_key, value)
        start_read = start_read + mm(read_remove, start)
        head_right = pick(right_tail)
        transit = transit + mm(start.T, head_right)
        added = added + mm(carried.T, head_right) + mm(value.T, pick(key_tail))
    return local_out, start_read, transit, added


def finish_unit(width, read, q, k, v, gain, own, gate):
    ones = same_head(width)
    mean = mm(read, ones) / width
    centered = read - mean
    variance = mm(centered * centered, ones) / width
    normed = centered * lax.rsqrt(variance + head_epsilon) * gain
    diagonal = mm(q * k * own, ones) * v
    return ((normed + diagonal) * gate).astype(jnp.bfloat16)


def members_of(n_sp):
    best = 1
    for count in range(1, n_sp + 1):
        if n_sp % count == 0 and count * count <= 2 * n_sp:
            best = count
    return best


def layer_kernel(
    n_sp, n_tp, widths, q_ref, k_ref, v_ref, f_ref, a_ref, e_ref, g_ref, gain_ref, own_ref,
    residual_ref, scale_ref, project_hbm, gate_hbm, up_hbm, down_hbm,
    out_ref,
    local_ref, read_ref, near, total_move, total_add, chain_in, chain_out, mixed_ref, project,
    wide, tall, pair_send, pair_got, term_send, term_got, hidden, active, summed,
    low_send, low_got, high_send, high_got, line_send, line_got,
    project_sem, keep_sem, out_sem, in_sem, pass_out, pass_in,
    near_out, near_in, chain_sem_out, chain_sem_in, pair_out, pair_in, term_out, term_in,
    row_out, row_in, up_out, up_in, side_out, side_in,
    low_out, low_in, high_out, high_in, line_out, line_in,
):
    F = members_of(n_sp)
    T = n_sp // F
    LO = 2 if n_tp % 2 == 0 else 1
    HI = n_tp // LO
    me = lax.axis_index("sp")
    t = lax.axis_index("tp")
    m, g = me // T, me % T
    hi, lo = t // LO, t % LO
    tokens = q_ref.shape[1]
    rows = gate_hbm.shape[0]
    depth = hidden.shape[1]
    own_cols = depth // n_tp
    down_cols = down_hbm.shape[1]
    base, extra = divmod(gate_hbm.shape[1] // LANES, F)
    parts = 2 if extra else 1

    def member(d):
        return lax.rem(m + d + F, F)

    def other(e):
        return lax.rem(g + e + T, T)

    def cell(h, l):
        return lax.rem(hi + h + HI, HI) * LO + lax.rem(lo + l + LO, LO)

    def remote(src, dst, send, recv, sp, tp):
        return pltpu.make_async_remote_copy(
            src_ref=src, dst_ref=dst, send_sem=send, recv_sem=recv,
            device_id=(sp, tp), device_id_type=MESH,
        )

    barrier = pltpu.get_barrier_semaphore()

    def greet(sp, tp):
        pl.semaphore_signal(barrier, inc=1, device_id=(sp, tp), device_id_type=MESH)

    for d in range(1, F):
        greet(member(d) * T + g, t)
    for e in range(1, T):
        greet(m * T + other(e), t)
    for d in range(1, n_tp):
        greet(me, lax.rem(t + d, n_tp))
    project_copy = pltpu.make_async_copy(project_hbm, project, project_sem)
    project_copy.start()
    pl.semaphore_wait(barrier, F + T + n_tp - 3)

    def more(dest):
        return jnp.where(t % 2 == 0, dest < extra, dest >= F - extra)

    def source(w, part, dest):
        before = jnp.where(t % 2 == 0, jnp.minimum(dest, extra), jnp.maximum(dest - F + extra, 0))
        tile = dest * base + before + (base if part else 0)
        at = pl.ds(pl.multiple_of(tile * LANES, LANES), LANES if part else base * LANES)
        return down_hbm.at[at, :] if w == 2 else (gate_hbm, up_hbm)[w].at[:, at]

    def landing(w, part, s):
        at = pl.ds(base * LANES if part else 0, LANES if part else base * LANES)
        if w == 2:
            return tall.at[s, at, :]
        return wide.at[w, pl.ds(pl.multiple_of(s * rows, rows), rows), at]

    def guarded(part, dest, action):
        if part:
            pl.when(more(dest))(action)
        else:
            action()

    def give(w, part, d):
        dest = member(d)
        return remote(
            source(w, part, dest), landing(w, part, me), out_sem.at[w, part, d],
            in_sem.at[w, part, d], dest * T + g, t,
        )

    def take(w, part, d):
        return remote(
            source(w, part, m), landing(w, part, member(-d) * T + g), out_sem.at[w, part, d],
            in_sem.at[w, part, d], me, t,
        )

    def hand(w, part, d, e):
        s = member(-d) * T + g
        src = source(w, part, m) if d == 0 else landing(w, part, s)
        return remote(
            src, landing(w, part, s), pass_out.at[w, part, d, e], pass_in.at[w, part, d, e],
            m * T + other(e), t,
        )

    def accept(w, part, d, e):
        s = member(-d) * T + other(-e)
        return remote(
            source(w, part, m), landing(w, part, s), pass_out.at[w, part, d, e],
            pass_in.at[w, part, d, e], me, t,
        )

    def keep(w, part):
        return pltpu.make_async_copy(
            source(w, part, m), landing(w, part, me), keep_sem.at[w, part]
        )

    def open_weight(w):
        for part in range(parts):

            def begin():
                keep(w, part).start()
                for e in range(1, T):
                    hand(w, part, 0, e).start()

            guarded(part, m, begin)

    def send_weight(w, chosen_parts):
        for part in chosen_parts:
            for upward, ways in ((True, range(F - 1, 0, -1)), (False, range(1, F))):
                for d in ways:
                    dest = member(d)
                    chosen = dest > m if upward else dest < m
                    if part:
                        chosen = chosen & more(dest)
                    pl.when(chosen)(lambda: give(w, part, d).start())

    def relay_weight(w, chosen_parts):
        for part in chosen_parts:
            for d in range(1, F):

                def pass_on():
                    take(w, part, d).wait_recv()
                    for e in range(1, T):
                        hand(w, part, d, e).start()

                guarded(part, m, pass_on)

    def arrived_weight(w):
        for part in range(parts):

            def settle():
                keep(w, part).wait()
                for d in range(F):
                    for e in range(1, T):
                        accept(w, part, d, e).wait_recv()

            guarded(part, m, settle)

    for w in range(2):
        open_weight(w)
        send_weight(w, range(parts))
    if extra:

        @pl.when(jnp.logical_not(more(m)))
        def _():
            tall[:, base * LANES :, :] = jnp.zeros(
                (n_sp, LANES, down_cols), jnp.bfloat16
            )

    per_group = q_ref.shape[2] // LANES

    def load(ref, group, c):
        return ref[group, :, c * LANES : (c + 1) * LANES].astype(jnp.float32)

    units = [(group, c) for group in range(2) for c in range(per_group)]

    def near_copy(u, e):
        return remote(
            near.at[g, u], near.at[g, u], near_out.at[u, e], near_in.at[u, e],
            m * T + other(e), t,
        )

    def near_take(u, e):
        return remote(
            near.at[other(-e), u], near.at[other(-e), u], near_out.at[u, e],
            near_in.at[u, e], me, t,
        )

    for u, (group, c) in enumerate(units):
        local_out, start_read, transit, added = local_unit(
            widths[group],
            *(load(r, group, c) for r in (q_ref, k_ref, v_ref, f_ref, a_ref, e_ref)),
        )
        local_ref[u] = local_out
        read_ref[u] = start_read
        near[g, u, 0] = transit.astype(jnp.bfloat16)
        near[g, u, 1] = added.astype(jnp.bfloat16)
    for u in range(len(units)):
        for e in range(1, T):
            near_copy(u, e).start()

    @pl.when(m == 0)
    def _():
        chain_in[...] = jnp.zeros_like(chain_in)

    relay_weight(0, range(parts))

    def chain_copy(u):
        return remote(
            chain_out.at[u], chain_in.at[u], chain_sem_out.at[u], chain_sem_in.at[u],
            member(1) * T + g, t,
        )

    for u in range(len(units)):
        for e in range(1, T):
            near_take(u, e).wait_recv()
        move, add = near[0, u, 0], near[0, u, 1].astype(jnp.float32)
        for other_g in range(1, T):
            step = near[other_g, u, 0]
            add = mm(add, step) + near[other_g, u, 1].astype(jnp.float32)
            move = mm(move, step).astype(jnp.bfloat16)
        total_move[u] = move
        total_add[u] = add
    for u in range(len(units)):

        @pl.when(m > 0)
        def _():
            chain_copy(u).wait_recv()

        following = mm(chain_in[u], total_move[u]) + total_add[u]
        chain_out[u] = following.astype(jnp.bfloat16)

        @pl.when(m < F - 1)
        def _():
            chain_copy(u).start()

    def fold(other_g, states):
        return tuple(
            mm(s, near[other_g, u, 0]) + near[other_g, u, 1].astype(jnp.float32)
            for u, s in enumerate(states)
        )

    states = lax.fori_loop(
        0, g, fold, tuple(chain_in[u].astype(jnp.float32) for u in range(len(units)))
    )
    for u, (group, c) in enumerate(units):
        lanes = slice(c * LANES, (c + 1) * LANES)
        read = local_ref[u] + mm_nt(read_ref[u], states[u])
        mixed_ref[:, u * LANES : (u + 1) * LANES] = finish_unit(
            widths[group], read, load(q_ref, group, c), load(k_ref, group, c),
            load(v_ref, group, c), gain_ref[group : group + 1, lanes],
            own_ref[group : group + 1, lanes], load(g_ref, group, c),
        )

    project_copy.wait()
    mixed = mixed_ref[...]

    def columns(at):
        return pl.ds(pl.multiple_of(at * own_cols, own_cols), own_cols)

    def term(at):
        return jnp.dot(mixed, project[:, columns(at)], preferred_element_type=jnp.float32)

    def pair_copy(h, l):
        return remote(
            pair_send.at[h, l], pair_got.at[h, l], pair_out.at[h, l], pair_in.at[h, l],
            me, cell(0, l),
        )

    def term_copy(h):
        return remote(
            term_send.at[h], term_got.at[h], term_out.at[h], term_in.at[h], me, cell(h, 0)
        )

    far = list(range(1, HI)) + [0]
    for h in far:
        for l in range(1, LO):
            pair_send[h, l] = term(cell(h, l)).astype(jnp.bfloat16)
            pair_copy(h, l).start()
    for h in far:
        branch = term(cell(h, 0))
        for l in range(1, LO):
            pair_copy(h, l).wait_recv()
            branch = branch + pair_got[h, l].astype(jnp.float32)
        if h:
            term_send[h] = branch.astype(jnp.bfloat16)
            term_copy(h).start()
    relay_weight(1, range(parts))
    for h in range(1, HI):
        term_copy(h).wait_recv()
        branch = branch + term_got[h].astype(jnp.float32)

    def positions(at):
        return pl.ds(pl.multiple_of(at * tokens, tokens), tokens)

    own_state = (residual_ref[:, columns(t)].astype(jnp.float32) + branch).astype(jnp.bfloat16)
    hidden[positions(m), columns(t)] = own_state

    def block(a, at):
        return hidden.at[positions(a), columns(at)]

    def row_copy(a, d):
        return remote(
            block(a, t), block(a, t), row_out.at[d], row_in.at[a], member(d) * T + g, t
        )

    def up_copy(a, h):
        return remote(block(a, t), block(a, t), up_out.at[a, h], up_in.at[a, h], me, cell(h, 0))

    def up_take(a, h):
        at = block(a, cell(-h, 0))
        return remote(at, at, up_out.at[a, h], up_in.at[a, h], me, t)

    def side_copy(a, h, l):
        at = block(a, cell(-h, 0))
        return remote(at, at, side_out.at[a, h, l], side_in.at[a, h, l], me, cell(0, l))

    def side_take(a, h, l):
        at = block(a, cell(-h, -l))
        return remote(at, at, side_out.at[a, h, l], side_in.at[a, h, l], me, t)

    def spread(a):
        for h in range(1, HI):
            up_copy(a, h).start()
        for l in range(1, LO):
            side_copy(a, 0, l).start()

    width = wide.shape[2]
    have = (base + more(m).astype(jnp.int32)) * LANES if extra else width

    def activate(a):
        state = hidden[positions(a), :].astype(jnp.float32)
        power = jnp.sum(state * state, axis=1, keepdims=True) / depth
        normed = (state * lax.rsqrt(power + norm_epsilon) * scale_ref[...]).astype(jnp.bfloat16)
        gate_pre = jnp.dot(normed, wide[0], preferred_element_type=jnp.float32)
        up_pre = jnp.dot(normed, wide[1], preferred_element_type=jnp.float32)
        value = gate_pre / (1.0 + jnp.exp(-gate_pre)) * up_pre
        if extra:
            lane = lax.broadcasted_iota(jnp.int32, (1, width), 1)
            value = jnp.where(lane < have, value, 0.0)
        active[positions(a), :] = value.astype(jnp.bfloat16)

    for d in range(1, F):
        pl.when(m + d < F)(lambda: row_copy(m, d).start())
    for d in range(1, F):
        pl.when(m + d >= F)(lambda: row_copy(m, d).start())
    spread(m)
    open_weight(2)
    send_weight(2, range(parts))

    @pl.loop(0, F + 2)
    def _(i):
        @pl.when((i < F) & (i != m))
        def _():
            row_copy(i, 0).wait_recv()
            spread(i)

        @pl.when((i >= 1) & (i <= F))
        def _():
            for h in range(1, HI):
                up_take(i - 1, h).wait_recv()
                for l in range(1, LO):
                    side_copy(i - 1, h, l).start()

        @pl.when(i == 2)
        def _():
            arrived_weight(0)
            arrived_weight(1)

        @pl.when(i >= 2)
        def _():
            for h in range(HI):
                for l in range(1, LO):
                    side_take(i - 2, h, l).wait_recv()
            activate(i - 2)

    relay_weight(2, range(parts))
    arrived_weight(2)

    def target(k):
        if k == F - 1:
            return m
        rising = k + (k >= m).astype(jnp.int32)
        falling = F - 1 - k - (F - 1 - k <= m).astype(jnp.int32)
        return jnp.where(2 * m >= F, rising, falling)

    def low_copy(k, h, l):
        return remote(
            low_send.at[k, h, l], low_got.at[k, h, l], low_out.at[k, h, l],
            low_in.at[k, h, l], me, cell(0, l),
        )

    def high_copy(k, h):
        return remote(
            high_send.at[k, h], high_got.at[k, h], high_out.at[k, h], high_in.at[k, h],
            me, cell(h, 0),
        )

    def line_copy(k):
        return remote(
            line_send.at[k], line_got.at[m], line_out.at[k], line_in.at[m],
            target(k) * T + g, t,
        )

    def line_take(a):
        return remote(line_send.at[0], line_got.at[a], line_out.at[0], line_in.at[a], me, t)

    for k in range(F):
        here = positions(target(k))
        units_here = active[here, :]
        for s in range(n_sp):
            summed[here, s * down_cols : (s + 1) * down_cols] = jnp.dot(
                units_here, tall[s], preferred_element_type=jnp.float32
            )
        for h in far:
            for l in range(1, LO):
                low_send[k, h, l] = summed[here, columns(cell(h, l))].astype(jnp.bfloat16)
                low_copy(k, h, l).start()

    def two_cores(k, h):
        value = summed[positions(target(k)), columns(cell(h, 0))]
        for l in range(1, LO):
            value = value + low_got[k, h, l].astype(jnp.float32)
        return value

    for k in range(F):
        for h in range(HI):
            for l in range(1, LO):
                low_copy(k, h, l).wait_recv()
        for h in range(1, HI):
            high_send[k, h] = two_cores(k, h).astype(jnp.bfloat16)
            high_copy(k, h).start()

    for k in range(F):
        value = two_cores(k, 0)
        for h in range(1, HI):
            high_copy(k, h).wait_recv()
            value = value + high_got[k, h].astype(jnp.float32)
        if k < F - 1:
            line_send[k] = value.astype(jnp.bfloat16)
            line_copy(k).start()
    summed[:tokens, :own_cols] = hidden[positions(m), columns(t)].astype(jnp.float32) + value

    @pl.loop(0, F)
    def _(a):
        @pl.when(a != m)
        def _():
            line_take(a).wait_recv()
            summed[:tokens, :own_cols] += line_got[a].astype(jnp.float32)

    out_ref[...] = summed[:tokens, :own_cols].astype(jnp.bfloat16)

    for w in range(3):
        for part in range(parts):
            for d in range(1, F):
                guarded(part, member(d), lambda: give(w, part, d).wait_send())

            def passed():
                for d in range(F):
                    for e in range(1, T):
                        hand(w, part, d, e).wait_send()

            guarded(part, m, passed)
    for u in range(len(units)):
        for e in range(1, T):
            near_copy(u, e).wait_send()

    @pl.when(m < F - 1)
    def _():
        for u in range(len(units)):
            chain_copy(u).wait_send()

    for h in range(HI):
        if h:
            term_copy(h).wait_send()
        for l in range(1, LO):
            pair_copy(h, l).wait_send()
    for d in range(F):
        if d:
            row_copy(m, d).wait_send()
            line_copy(d - 1).wait_send()
        for h in range(HI):
            if h:
                up_copy(d, h).wait_send()
                high_copy(d, h).wait_send()
            for l in range(1, LO):
                side_copy(d, h, l).wait_send()
                low_copy(d, h, l).wait_send()


def layer(n_sp, n_tp, q, k, v, f, a, e, g, gain, own, residual, scale, project, gate, up, down):
    tokens, channels = q.shape[1], q.shape[2]
    units = 2 * channels // LANES
    depth = residual.shape[1]
    cols = depth // n_tp
    F = members_of(n_sp)
    T = n_sp // F
    LO = 2 if n_tp % 2 == 0 else 1
    HI = n_tp // LO
    width = -(-(gate.shape[1] // LANES) // F) * LANES
    vmem = pl.BlockSpec(memory_space=pltpu.VMEM)
    hbm = pl.BlockSpec(memory_space=pl.ANY)
    bf16, f32 = jnp.bfloat16, jnp.float32
    sem = pltpu.SemaphoreType.DMA
    scratch = [
        pltpu.VMEM((units, tokens, LANES), f32),
        pltpu.VMEM((units, tokens, LANES), f32),
        pltpu.VMEM((T, units, 2, LANES, LANES), bf16),
        pltpu.VMEM((units, LANES, LANES), bf16),
        pltpu.VMEM((units, LANES, LANES), f32),
        pltpu.VMEM((units, LANES, LANES), bf16),
        pltpu.VMEM((units, LANES, LANES), bf16),
        pltpu.VMEM((tokens, units * LANES), bf16),
        pltpu.VMEM(project.shape, bf16),
        pltpu.VMEM((2, depth, width), bf16),
        pltpu.VMEM((n_sp, width, down.shape[1]), bf16),
        pltpu.VMEM((HI, LO, tokens, cols), bf16),
        pltpu.VMEM((HI, LO, tokens, cols), bf16),
        pltpu.VMEM((HI, tokens, cols), bf16),
        pltpu.VMEM((HI, tokens, cols), bf16),
        pltpu.VMEM((F * tokens, depth), bf16),
        pltpu.VMEM((F * tokens, width), bf16),
        pltpu.VMEM((F * tokens, depth), f32),
        pltpu.VMEM((F, HI, LO, tokens, cols), bf16),
        pltpu.VMEM((F, HI, LO, tokens, cols), bf16),
        pltpu.VMEM((F, HI, tokens, cols), bf16),
        pltpu.VMEM((F, HI, tokens, cols), bf16),
        pltpu.VMEM((F, tokens, cols), bf16),
        pltpu.VMEM((F, tokens, cols), bf16),
        sem, sem((3, 2)),
    ]
    for shape in (
        (3, 2, F), (3, 2, F, T), (units, T), (units,), (HI, LO), (HI,), (F,), (F, HI), (F, HI, LO),
        (F, HI, LO), (F, HI), (F,),
    ):
        scratch += [sem(shape), sem(shape)]
    return pl.pallas_call(
        functools.partial(layer_kernel, n_sp, n_tp, (DS, DL)),
        out_shape=jax.ShapeDtypeStruct((tokens, cols), bf16),
        in_specs=[vmem] * 11 + [hbm] * 4,
        out_specs=vmem,
        scratch_shapes=scratch,
        compiler_params=pltpu.CompilerParams(
            collective_id=0, has_side_effects=True, vmem_limit_bytes=60 * 2**20
        ),
        name="layer",
    )(q, k, v, f, a, e, g, gain, own, residual, scale, project, gate, up, down)


def on_device(
    stratum_source_matrix,
    acceptance_query,
    cluster_lookup_matrix,
    cluster_payload_matrix,
    fading_logit,
    adaptation_speed_logit,
    additional_fading_exponent,
    result_switch_pair,
    attender_scaling_factor,
    present_item_factor,
    final_mapping_matrix,
    perceptron_scaling_factor,
    switching_matrix,
    widening_matrix,
    shrinking_matrix,
):
    return layer(
        lax.axis_size("sp"),
        lax.axis_size("tp"),
        acceptance_query,
        cluster_lookup_matrix,
        cluster_payload_matrix,
        fading_logit,
        adaptation_speed_logit,
        additional_fading_exponent,
        result_switch_pair,
        attender_scaling_factor,
        present_item_factor,
        stratum_source_matrix,
        perceptron_scaling_factor.reshape(1, -1),
        final_mapping_matrix.reshape(-1, final_mapping_matrix.shape[2]),
        switching_matrix,
        widening_matrix,
        shrinking_matrix,
    )


def solution(mesh):
    tokens = P(None, "sp", "tp")
    in_specs = (
        P("sp", None), tokens, tokens, tokens, tokens, tokens, tokens, tokens,
        P(None, "tp"), P(None, "tp"), P(None, "tp", None), P(),
        P("sp", "tp"), P("sp", "tp"), P("tp", "sp"),
    )
    return jax.shard_map(
        on_device, mesh=mesh, in_specs=in_specs, out_specs=P("sp", "tp"), check_vma=False
    )
```

```python
import functools

import jax
import jax.numpy as jnp
from jax import lax
from jax.experimental import pallas as pl
from jax.experimental.pallas import tpu as pltpu
from jax.sharding import PartitionSpec as P

DS = 64
DL = 128
LANES = 128
MESH = pl.DeviceIdType.MESH

norm_epsilon = 1e-06
head_epsilon = 0.00064
key_epsilon = 1e-06


NN = (((1,), (0,)), ((), ()))
NT = (((1,), (1,)), ((), ()))
TN = (((0,), (0,)), ((), ()))


def split(x, count=2):
    if x.dtype == jnp.bfloat16:
        return [x]
    parts = []
    for _ in range(count - 1):
        high = x.astype(jnp.bfloat16)
        parts.append(high)
        x = x - high.astype(jnp.float32)
    return parts + [x.astype(jnp.bfloat16)]


def product(a, b, dims, count=2):
    total = None
    for i, p in enumerate(split(a, count)):
        for j, r in enumerate(split(b, count)):
            if i + j < count:
                term = lax.dot_general(p, r, dims, preferred_element_type=jnp.float32)
                total = term if total is None else total + term
    return total


def mm(a, b, count=2):
    return product(a, b, NN, count)


def mm_nt(a, b):
    return product(a, b, NT)


def sigmoid(x):
    return 1.0 / (1.0 + jnp.exp(-x))


def same_head(width):
    i = lax.broadcasted_iota(jnp.int32, (LANES, LANES), 0) // width
    j = lax.broadcasted_iota(jnp.int32, (LANES, LANES), 1) // width
    return (i == j).astype(jnp.float32).astype(jnp.bfloat16)


def pair_up(a, b):
    zero = jnp.zeros_like(a)
    return jnp.concatenate(
        [jnp.concatenate([a, zero], axis=1), jnp.concatenate([zero, b], axis=1)], axis=0
    )


def unit_inverses(strict_parts, rows, cols):
    size = strict_parts[0].shape[0]
    pairs = [strict_parts[i : i + 2] for i in range(0, len(strict_parts), 2)]
    eye = (rows == cols).astype(jnp.float32)
    inverses = None
    half = 1
    while half < size:
        off = (rows // (2 * half) == cols // (2 * half)) & (rows // half != cols // half)
        parts = [[jnp.where(off, s, 0.0) for s in pair] for pair in pairs]
        if half == 1:
            inverses = [jnp.concatenate([eye + p for p in pair], axis=1) for pair in parts]
        else:
            middles = [
                product_of(split(inverse), [pair_up(*x) for x in zip(*(split(p) for p in pair))])
                for inverse, pair in zip(inverses, parts)
            ]
            inverses = [
                inverse
                + product_of(
                    split(middle),
                    [pair_up(x[:, :size], x[:, size:]) for x in split(inverse)],
                )
                for inverse, middle in zip(inverses, middles)
            ]
        half *= 2
    return [inverse[:, i * size : (i + 1) * size] for inverse in inverses for i in range(2)]


def product_of(left, right, dims=NN):
    total = None
    for i, p in enumerate(left):
        for j, r in enumerate(right):
            if i + j < 2:
                term = lax.dot_general(p, r, dims, preferred_element_type=jnp.float32)
                total = term if total is None else total + term
    return total


def local_units(widths, tokens):
    T = tokens[0][0].shape[0]
    rows = lax.broadcasted_iota(jnp.int32, (T, T), 0)
    cols = lax.broadcasted_iota(jnp.int32, (T, T), 1)
    inclusive = rows >= cols
    strict = rows > cols
    running = inclusive.astype(jnp.float32).astype(jnp.bfloat16)
    eye = lax.broadcasted_iota(jnp.int32, (LANES, LANES), 0) == lax.broadcasted_iota(
        jnp.int32, (LANES, LANES), 1
    )
    decays = [t[5] - jnp.exp(jnp.float32(-0.5)) * sigmoid(t[3].astype(jnp.float32)) for t in tokens]
    cumulatives = [mm(running, d, 3) for d in decays]
    heads, units = [], []
    for width, (q, k, v, fade, speed, extra), log_decay, cumulative in zip(
        widths, tokens, decays, cumulatives
    ):
        q, k = q.astype(jnp.float32), k.astype(jnp.float32)
        removal = k * lax.rsqrt(mm(k * k, same_head(width)) + key_epsilon)
        left = -removal
        right = sigmoid(speed.astype(jnp.float32)) * removal
        middle = cumulative[T // 2 : T // 2 + 1, :]
        final = cumulative[T - 1 : T, :]
        forward = jnp.exp(cumulative - middle)
        backward = jnp.exp(middle - cumulative)
        tail = jnp.exp(final - cumulative)
        queries = split(jnp.concatenate([left * jnp.exp(-log_decay) * forward, q * forward], axis=0))
        sources = split(jnp.concatenate([right * backward, k * backward], axis=0))
        start_target = left * jnp.exp(cumulative - log_decay)
        right_tail = split(right * tail)
        key_tail = split(k * tail)
        units.append([
            jnp.zeros((T, LANES), jnp.float32),
            q * jnp.exp(cumulative),
            jnp.where(eye, jnp.exp(final), 0.0),
            jnp.zeros((LANES, LANES), jnp.float32),
        ])
        lane = lax.broadcasted_iota(jnp.int32, (1, LANES), 1) // width
        for head in range(LANES // width):
            if width == LANES:
                pick = lambda a: a
            else:
                pick = lambda a, only=lane == head: jnp.where(only, a, jnp.zeros_like(a))
            heads.append((
                len(units) - 1, pick(v), pick(start_target), [pick(x) for x in right_tail],
                [pick(x) for x in key_tail],
                product_of([pick(x) for x in queries], sources, NT),
            ))
    inverses = unit_inverses(
        [jnp.where(strict, h[5][:T, :T], 0.0) for h in heads], rows, cols
    )
    for (u, value, target, head_right, head_key, pairs), inverse in zip(heads, inverses):
        remove_key = jnp.where(strict, pairs[:T, T:], 0.0)
        read_remove = jnp.where(inclusive, pairs[T:, :T], 0.0)
        read_key = jnp.where(inclusive, pairs[T:, T:], 0.0)
        both = mm(inverse, jnp.concatenate([mm(remove_key, value), target], axis=1))
        reads = mm(read_remove, both)
        moved = product_of(split(both), head_right, TN)
        units[u][0] = units[u][0] + reads[:, :LANES] + mm(read_key, value)
        units[u][1] = units[u][1] + reads[:, LANES:]
        units[u][2] = units[u][2] + moved[LANES:]
        units[u][3] = units[u][3] + moved[:LANES] + product_of([value], head_key, TN)
    return units


def finish_unit(width, read, q, k, v, gain, own, gate):
    ones = same_head(width)
    mean = mm(read, ones) / width
    centered = read - mean
    variance = mm(centered * centered, ones) / width
    normed = centered * lax.rsqrt(variance + head_epsilon) * gain
    diagonal = mm(q * k * own, ones) * v
    return ((normed + diagonal) * gate).astype(jnp.bfloat16)


def members_of(n_sp):
    best = 1
    for count in range(1, n_sp + 1):
        if n_sp % count == 0 and count * count <= 2 * n_sp:
            best = count
    return best


def layer_kernel(
    n_sp, n_tp, widths, q_ref, k_ref, v_ref, f_ref, a_ref, e_ref, g_ref, gain_ref, own_ref,
    residual_ref, scale_ref, project_hbm, gate_hbm, up_hbm, down_hbm,
    out_ref,
    local_ref, read_ref, near, total_move, total_add, chain_in, chain_out, mixed_ref, project,
    total, wide, tall, pair_send, pair_got, term_send, term_got, hidden, active, summed,
    low_send, low_got, high_send, high_got, line_send, line_got,
    project_sem, keep_sem, out_sem, in_sem, pass_out, pass_in,
    near_out, near_in, chain_sem_out, chain_sem_in, pair_out, pair_in, term_out, term_in,
    row_out, row_in, up_out, up_in, side_out, side_in,
    low_out, low_in, high_out, high_in, line_out, line_in,
):
    F = members_of(n_sp)
    T = n_sp // F
    LO = 2 if n_tp % 2 == 0 else 1
    HI = n_tp // LO
    me = lax.axis_index("sp")
    t = lax.axis_index("tp")
    m, g = me // T, me % T
    hi, lo = t // LO, t % LO
    tokens = q_ref.shape[1]
    rows = gate_hbm.shape[0]
    depth = hidden.shape[1]
    own_cols = depth // n_tp
    down_cols = down_hbm.shape[1]
    base, extra = divmod(gate_hbm.shape[1] // LANES, F)
    parts = 2 if extra else 1

    def member(d):
        return lax.rem(m + d + F, F)

    def other(e):
        return lax.rem(g + e + T, T)

    def cell(h, l):
        return lax.rem(hi + h + HI, HI) * LO + lax.rem(lo + l + LO, LO)

    def remote(src, dst, send, recv, sp, tp):
        return pltpu.make_async_remote_copy(
            src_ref=src, dst_ref=dst, send_sem=send, recv_sem=recv,
            device_id=(sp, tp), device_id_type=MESH,
        )

    barrier = pltpu.get_barrier_semaphore()

    def greet(sp, tp):
        pl.semaphore_signal(barrier, inc=1, device_id=(sp, tp), device_id_type=MESH)

    for d in range(1, F):
        greet(member(d) * T + g, t)
    for e in range(1, T):
        greet(m * T + other(e), t)
    for d in range(1, n_tp):
        greet(me, lax.rem(t + d, n_tp))
    project_copy = pltpu.make_async_copy(project_hbm, project, project_sem)
    project_copy.start()
    pl.semaphore_wait(barrier, F + T + n_tp - 3)

    def more(dest):
        return jnp.where(t % 2 == 0, dest < extra, dest >= F - extra)

    def source(w, part, dest):
        before = jnp.where(t % 2 == 0, jnp.minimum(dest, extra), jnp.maximum(dest - F + extra, 0))
        tile = dest * base + before + (base if part else 0)
        at = pl.ds(pl.multiple_of(tile * LANES, LANES), LANES if part else base * LANES)
        return down_hbm.at[at, :] if w == 2 else (gate_hbm, up_hbm)[w].at[:, at]

    def landing(w, part, s):
        at = pl.ds(base * LANES if part else 0, LANES if part else base * LANES)
        if w == 2:
            return tall.at[s, at, :]
        return wide.at[w, pl.ds(pl.multiple_of(s * rows, rows), rows), at]

    def guarded(part, dest, action):
        if part:
            pl.when(more(dest))(action)
        else:
            action()

    def give(w, part, d):
        dest = member(d)
        return remote(
            source(w, part, dest), landing(w, part, me), out_sem.at[w, part, d],
            in_sem.at[w, part, d], dest * T + g, t,
        )

    def take(w, part, d):
        return remote(
            source(w, part, m), landing(w, part, member(-d) * T + g), out_sem.at[w, part, d],
            in_sem.at[w, part, d], me, t,
        )

    def hand(w, part, d, e):
        s = member(-d) * T + g
        src = source(w, part, m) if d == 0 else landing(w, part, s)
        return remote(
            src, landing(w, part, s), pass_out.at[w, part, d, e], pass_in.at[w, part, d, e],
            m * T + other(e), t,
        )

    def accept(w, part, d, e):
        s = member(-d) * T + other(-e)
        return remote(
            source(w, part, m), landing(w, part, s), pass_out.at[w, part, d, e],
            pass_in.at[w, part, d, e], me, t,
        )

    def keep(w, part):
        return pltpu.make_async_copy(
            source(w, part, m), landing(w, part, me), keep_sem.at[w, part]
        )

    def open_weight(w):
        for part in range(parts):

            def begin():
                keep(w, part).start()
                for e in range(1, T):
                    hand(w, part, 0, e).start()

            guarded(part, m, begin)

    def send_part(w, part, d, upward):
        dest = member(d)
        chosen = dest > m if upward else dest < m
        if part:
            chosen = chosen & more(dest)
        pl.when(chosen)(lambda: give(w, part, d).start())

    def send_weight(w, upward, chosen_parts):
        for part in chosen_parts:
            for d in range(F - 1, 0, -1) if upward else range(1, F):
                send_part(w, part, d, upward)

    def send_near_first(w, upward, chosen_parts):
        for d in range(1, F) if upward else range(F - 1, 0, -1):
            for part in chosen_parts:
                send_part(w, part, d, upward)

    def relay_weight(w, chosen_parts):
        for part in chosen_parts:
            for d in range(1, F):

                def pass_on():
                    take(w, part, d).wait_recv()
                    for e in range(1, T):
                        hand(w, part, d, e).start()

                guarded(part, m, pass_on)

    def arrived_weight(w):
        for part in range(parts):

            def settle():
                keep(w, part).wait()
                for d in range(F):
                    for e in range(1, T):
                        accept(w, part, d, e).wait_recv()

            guarded(part, m, settle)

    every, first, rest = range(parts), range(1), range(1, parts)
    open_weight(0)
    send_weight(0, True, every)
    send_weight(0, False, every)
    send_weight(1, False, every)
    send_weight(2, False, first)
    if extra:

        @pl.when(jnp.logical_not(more(m)))
        def _():
            tall[:, base * LANES :, :] = jnp.zeros(
                (n_sp, LANES, down_cols), jnp.bfloat16
            )

    per_group = q_ref.shape[2] // LANES

    def load(ref, group, c):
        return ref[group, :, c * LANES : (c + 1) * LANES].astype(jnp.float32)

    units = [(group, c) for group in range(2) for c in range(per_group)]

    def near_copy(u, e):
        return remote(
            near.at[g, u], near.at[g, u], near_out.at[u, e], near_in.at[u, e],
            m * T + other(e), t,
        )

    def near_take(u, e):
        return remote(
            near.at[other(-e), u], near.at[other(-e), u], near_out.at[u, e],
            near_in.at[u, e], me, t,
        )

    def blocks(group, c):
        lanes = slice(c * LANES, (c + 1) * LANES)
        return [r[group, :, lanes] for r in (q_ref, k_ref, v_ref, f_ref, a_ref, e_ref)]

    local = local_units([widths[group] for group, _ in units], [blocks(*unit) for unit in units])
    for u, (local_out, start_read, transit, added) in enumerate(local):
        local_ref[u] = local_out
        read_ref[u] = start_read
        near[g, u, 0] = transit.astype(jnp.bfloat16)
        near[g, u, 1] = added.astype(jnp.bfloat16)
    for u in range(len(units)):
        for e in range(1, T):
            near_copy(u, e).start()

    @pl.when(m == 0)
    def _():
        chain_in[...] = jnp.zeros_like(chain_in)

    open_weight(1)
    open_weight(2)

    def chain_copy(u):
        return remote(
            chain_out.at[u], chain_in.at[u], chain_sem_out.at[u], chain_sem_in.at[u],
            member(1) * T + g, t,
        )

    for u in range(len(units)):
        for e in range(1, T):
            near_take(u, e).wait_recv()
        move, add = near[0, u, 0], near[0, u, 1].astype(jnp.float32)
        for other_g in range(1, T):
            step = near[other_g, u, 0]
            add = mm(add, step) + near[other_g, u, 1].astype(jnp.float32)
            move = mm(move, step).astype(jnp.bfloat16)
        total_move[u] = move
        total_add[u] = add
    for u in range(len(units)):

        @pl.when(m > 0)
        def _():
            chain_copy(u).wait_recv()

        following = mm(chain_in[u], total_move[u]) + total_add[u]
        chain_out[u] = following.astype(jnp.bfloat16)

        @pl.when(m < F - 1)
        def _():
            chain_copy(u).start()

    send_near_first(1, True, every)
    send_near_first(2, True, first)
    relay_weight(0, range(parts))

    def fold(other_g, states):
        return tuple(
            mm(s, near[other_g, u, 0]) + near[other_g, u, 1].astype(jnp.float32)
            for u, s in enumerate(states)
        )

    states = lax.fori_loop(
        0, g, fold, tuple(chain_in[u].astype(jnp.float32) for u in range(len(units)))
    )
    for u, (group, c) in enumerate(units):
        lanes = slice(c * LANES, (c + 1) * LANES)
        read = local_ref[u] + mm_nt(read_ref[u], states[u])
        mixed_ref[:, u * LANES : (u + 1) * LANES] = finish_unit(
            widths[group], read, load(q_ref, group, c), load(k_ref, group, c),
            load(v_ref, group, c), gain_ref[group : group + 1, lanes],
            own_ref[group : group + 1, lanes], load(g_ref, group, c),
        )

    project_copy.wait()
    mixed = mixed_ref[...]

    def columns(at):
        return pl.ds(pl.multiple_of(at * own_cols, own_cols), own_cols)

    def term(at):
        return jnp.dot(mixed, project[:, columns(at)], preferred_element_type=jnp.float32)

    def pair_copy(h, l):
        return remote(
            pair_send.at[h, l], pair_got.at[h, l], pair_out.at[h, l], pair_in.at[h, l],
            me, cell(0, l),
        )

    def term_copy(h):
        return remote(
            term_send.at[h], term_got.at[h], term_out.at[h], term_in.at[h], me, cell(h, 0)
        )

    far = list(range(1, HI)) + [0]
    for h in far:
        for l in range(1, LO):
            pair_send[h, l] = term(cell(h, l)).astype(jnp.bfloat16)
            pair_copy(h, l).start()
    for h in far:
        branch = term(cell(h, 0))
        for l in range(1, LO):
            pair_copy(h, l).wait_recv()
            branch = branch + pair_got[h, l].astype(jnp.float32)
        if h:
            term_send[h] = branch.astype(jnp.bfloat16)
            term_copy(h).start()
    for h in range(1, HI):
        term_copy(h).wait_recv()
        branch = branch + term_got[h].astype(jnp.float32)

    def positions(at):
        return pl.ds(pl.multiple_of(at * tokens, tokens), tokens)

    own_state = (residual_ref[:, columns(t)].astype(jnp.float32) + branch).astype(jnp.bfloat16)
    hidden[positions(m), columns(t)] = own_state

    def block(a, at):
        return hidden.at[positions(a), columns(at)]

    def row_copy(a, d):
        return remote(
            block(a, t), block(a, t), row_out.at[d], row_in.at[a], member(d) * T + g, t
        )

    def up_copy(a, h):
        return remote(block(a, t), block(a, t), up_out.at[a, h], up_in.at[a, h], me, cell(h, 0))

    def up_take(a, h):
        at = block(a, cell(-h, 0))
        return remote(at, at, up_out.at[a, h], up_in.at[a, h], me, t)

    def side_copy(a, h, l):
        at = block(a, cell(-h, 0))
        return remote(at, at, side_out.at[a, h, l], side_in.at[a, h, l], me, cell(0, l))

    def side_take(a, h, l):
        at = block(a, cell(-h, -l))
        return remote(at, at, side_out.at[a, h, l], side_in.at[a, h, l], me, t)

    def spread(a):
        for h in range(1, HI):
            up_copy(a, h).start()
        for l in range(1, LO):
            side_copy(a, 0, l).start()

    width = wide.shape[2]
    have = (base + more(m).astype(jnp.int32)) * LANES if extra else width

    def activate(a):
        state = hidden[positions(a), :].astype(jnp.float32)
        power = jnp.sum(state * state, axis=1, keepdims=True) / depth
        normed = (state * lax.rsqrt(power + norm_epsilon) * scale_ref[...]).astype(jnp.bfloat16)
        gate_pre = jnp.dot(normed, wide[0], preferred_element_type=jnp.float32)
        up_pre = jnp.dot(normed, wide[1], preferred_element_type=jnp.float32)
        value = gate_pre / (1.0 + jnp.exp(-gate_pre)) * up_pre
        if extra:
            lane = lax.broadcasted_iota(jnp.int32, (1, width), 1)
            value = jnp.where(lane < have, value, 0.0)
        active[positions(a), :] = value.astype(jnp.bfloat16)

    for d in range(1, F):
        pl.when(m + d < F)(lambda: row_copy(m, d).start())
    for d in range(1, F):
        pl.when(m + d >= F)(lambda: row_copy(m, d).start())
    spread(m)
    send_weight(2, True, rest)
    send_weight(2, False, rest)
    relay_weight(1, range(parts))

    def turn(k):
        return jnp.where(k == 0, m, k - 1 + (k - 1 >= m).astype(jnp.int32))

    def target(k):
        rising = k + (k >= m).astype(jnp.int32)
        falling = F - 1 - k - (F - 1 - k <= m).astype(jnp.int32)
        return jnp.where(k == F - 1, m, jnp.where(2 * m >= F, rising, falling))

    def low_copy(k, h, l):
        return remote(
            low_send.at[k, h, l], low_got.at[k, h, l], low_out.at[k, h, l],
            low_in.at[k, h, l], me, cell(0, l),
        )

    def high_copy(k, h):
        return remote(
            high_send.at[k, h], high_got.at[k, h], high_out.at[k, h], high_in.at[k, h],
            me, cell(h, 0),
        )

    def line_copy(k):
        return remote(
            line_send.at[k], line_got.at[m], line_out.at[k], line_in.at[m], target(k) * T + g, t
        )

    def line_take(a):
        return remote(line_send.at[0], line_got.at[a], line_out.at[0], line_in.at[a], me, t)

    def across(k):
        for h in range(1, HI):
            up_take(turn(k), h).wait_recv()
            for l in range(1, LO):
                side_copy(turn(k), h, l).start()

    def gathered(k):
        for h in range(HI):
            for l in range(1, LO):
                side_take(turn(k), h, l).wait_recv()
        activate(turn(k))

    def contract(k):
        here = positions(target(k))
        units_here = active[here, :]
        for s in range(n_sp):
            summed[here, s * down_cols : (s + 1) * down_cols] = jnp.dot(
                units_here, tall[s], preferred_element_type=jnp.float32
            )
        for h in far:
            for l in range(1, LO):
                low_send[k, h, l] = summed[here, columns(cell(h, l))].astype(jnp.bfloat16)
                low_copy(k, h, l).start()

    def two_cores(k, h):
        value = summed[positions(target(k)), columns(cell(h, 0))]
        for l in range(1, LO):
            value = value + low_got[k, h, l].astype(jnp.float32)
        return value

    def halve(k):
        for h in range(HI):
            for l in range(1, LO):
                low_copy(k, h, l).wait_recv()
        for h in range(1, HI):
            high_send[k, h] = two_cores(k, h).astype(jnp.bfloat16)
            high_copy(k, h).start()

    def whole(k):
        value = two_cores(k, 0)
        for h in range(1, HI):
            high_copy(k, h).wait_recv()
            value = value + high_got[k, h].astype(jnp.float32)
        return value

    relay_weight(2, range(1))
    across(0)

    @pl.loop(1, F + 1)
    def _(i):
        @pl.when(i < F)
        def _():
            row_copy(turn(i), 0).wait_recv()
            spread(turn(i))

        @pl.when(i >= 2)
        def _():
            across(i - 1)

    relay_weight(2, range(1, parts))
    arrived_weight(0)
    arrived_weight(1)

    @pl.loop(0, F)
    def _(k):
        gathered(k)

    arrived_weight(2)

    @pl.loop(0, F)
    def _(k):
        contract(k)

    @pl.loop(0, F)
    def _(k):
        halve(k)

    @pl.loop(0, F - 1)
    def _(k):
        line_send[k] = whole(k).astype(jnp.bfloat16)
        line_copy(k).start()

    total[...] = hidden[positions(m), columns(t)].astype(jnp.float32) + whole(F - 1)

    @pl.loop(0, F)
    def _(a):
        @pl.when(a != m)
        def _():
            line_take(a).wait_recv()
            total[...] += line_got[a].astype(jnp.float32)

    out_ref[...] = total[...].astype(jnp.bfloat16)

    for w in range(3):
        for part in range(parts):
            for d in range(1, F):
                guarded(part, member(d), lambda: give(w, part, d).wait_send())

            def passed():
                for d in range(F):
                    for e in range(1, T):
                        hand(w, part, d, e).wait_send()

            guarded(part, m, passed)
    for u in range(len(units)):
        for e in range(1, T):
            near_copy(u, e).wait_send()

    @pl.when(m < F - 1)
    def _():
        for u in range(len(units)):
            chain_copy(u).wait_send()

    for h in range(HI):
        if h:
            term_copy(h).wait_send()
        for l in range(1, LO):
            pair_copy(h, l).wait_send()
    for d in range(F):
        if d:
            row_copy(m, d).wait_send()
            line_copy(d - 1).wait_send()
        for h in range(HI):
            if h:
                up_copy(d, h).wait_send()
                high_copy(d, h).wait_send()
            for l in range(1, LO):
                side_copy(d, h, l).wait_send()
                low_copy(d, h, l).wait_send()


def layer(n_sp, n_tp, q, k, v, f, a, e, g, gain, own, residual, scale, project, gate, up, down):
    tokens, channels = q.shape[1], q.shape[2]
    units = 2 * channels // LANES
    depth = residual.shape[1]
    cols = depth // n_tp
    F = members_of(n_sp)
    T = n_sp // F
    LO = 2 if n_tp % 2 == 0 else 1
    HI = n_tp // LO
    width = -(-(gate.shape[1] // LANES) // F) * LANES
    vmem = pl.BlockSpec(memory_space=pltpu.VMEM)
    hbm = pl.BlockSpec(memory_space=pl.ANY)
    bf16, f32 = jnp.bfloat16, jnp.float32
    sem = pltpu.SemaphoreType.DMA
    scratch = [
        pltpu.VMEM((units, tokens, LANES), f32),
        pltpu.VMEM((units, tokens, LANES), f32),
        pltpu.VMEM((T, units, 2, LANES, LANES), bf16),
        pltpu.VMEM((units, LANES, LANES), bf16),
        pltpu.VMEM((units, LANES, LANES), f32),
        pltpu.VMEM((units, LANES, LANES), bf16),
        pltpu.VMEM((units, LANES, LANES), bf16),
        pltpu.VMEM((tokens, units * LANES), bf16),
        pltpu.VMEM(project.shape, bf16),
        pltpu.VMEM((tokens, cols), f32),
        pltpu.VMEM((2, depth, width), bf16),
        pltpu.VMEM((n_sp, width, down.shape[1]), bf16),
        pltpu.VMEM((HI, LO, tokens, cols), bf16),
        pltpu.VMEM((HI, LO, tokens, cols), bf16),
        pltpu.VMEM((HI, tokens, cols), bf16),
        pltpu.VMEM((HI, tokens, cols), bf16),
        pltpu.VMEM((F * tokens, depth), bf16),
        pltpu.VMEM((F * tokens, width), bf16),
        pltpu.VMEM((F * tokens, depth), f32),
        pltpu.VMEM((F, HI, LO, tokens, cols), bf16),
        pltpu.VMEM((F, HI, LO, tokens, cols), bf16),
        pltpu.VMEM((F, HI, tokens, cols), bf16),
        pltpu.VMEM((F, HI, tokens, cols), bf16),
        pltpu.VMEM((F, tokens, cols), bf16),
        pltpu.VMEM((F, tokens, cols), bf16),
        sem, sem((3, 2)),
    ]
    for shape in (
        (3, 2, F), (3, 2, F, T), (units, T), (units,), (HI, LO), (HI,), (F,), (F, HI), (F, HI, LO),
        (F, HI, LO), (F, HI), (F,),
    ):
        scratch += [sem(shape), sem(shape)]
    return pl.pallas_call(
        functools.partial(layer_kernel, n_sp, n_tp, (DS, DL)),
        out_shape=jax.ShapeDtypeStruct((tokens, cols), bf16),
        in_specs=[vmem] * 11 + [hbm] * 4,
        out_specs=vmem,
        scratch_shapes=scratch,
        compiler_params=pltpu.CompilerParams(
            collective_id=0, has_side_effects=True, vmem_limit_bytes=60 * 2**20
        ),
        name="layer",
    )(q, k, v, f, a, e, g, gain, own, residual, scale, project, gate, up, down)


def on_device(
    stratum_source_matrix,
    acceptance_query,
    cluster_lookup_matrix,
    cluster_payload_matrix,
    fading_logit,
    adaptation_speed_logit,
    additional_fading_exponent,
    result_switch_pair,
    attender_scaling_factor,
    present_item_factor,
    final_mapping_matrix,
    perceptron_scaling_factor,
    switching_matrix,
    widening_matrix,
    shrinking_matrix,
):
    return layer(
        lax.axis_size("sp"),
        lax.axis_size("tp"),
        acceptance_query,
        cluster_lookup_matrix,
        cluster_payload_matrix,
        fading_logit,
        adaptation_speed_logit,
        additional_fading_exponent,
        result_switch_pair,
        attender_scaling_factor,
        present_item_factor,
        stratum_source_matrix,
        perceptron_scaling_factor.reshape(1, -1),
        final_mapping_matrix.reshape(-1, final_mapping_matrix.shape[2]),
        switching_matrix,
        widening_matrix,
        shrinking_matrix,
    )


def solution(mesh):
    tokens = P(None, "sp", "tp")
    in_specs = (
        P("sp", None), tokens, tokens, tokens, tokens, tokens, tokens, tokens,
        P(None, "tp"), P(None, "tp"), P(None, "tp", None), P(),
        P("sp", "tp"), P("sp", "tp"), P("tp", "sp"),
    )
    return jax.shard_map(
        on_device, mesh=mesh, in_specs=in_specs, out_specs=P("sp", "tp"), check_vma=False
    )
```

```python
import functools

import jax
import jax.numpy as jnp
from jax import lax
from jax.experimental import pallas as pl
from jax.experimental.pallas import tpu as pltpu
from jax.sharding import PartitionSpec as P

DS = 64
DL = 128
LANES = 128
MESH = pl.DeviceIdType.MESH

norm_epsilon = 1e-06
head_epsilon = 0.00064
key_epsilon = 1e-06


NN = (((1,), (0,)), ((), ()))
NT = (((1,), (1,)), ((), ()))
TN = (((0,), (0,)), ((), ()))


def split(x, count=2):
    if x.dtype == jnp.bfloat16:
        return [x]
    parts = []
    for _ in range(count - 1):
        high = x.astype(jnp.bfloat16)
        parts.append(high)
        x = x - high.astype(jnp.float32)
    return parts + [x.astype(jnp.bfloat16)]


def product(a, b, dims, count=2):
    total = None
    for i, p in enumerate(split(a, count)):
        for j, r in enumerate(split(b, count)):
            if i + j < count:
                term = lax.dot_general(p, r, dims, preferred_element_type=jnp.float32)
                total = term if total is None else total + term
    return total


def mm(a, b, count=2):
    return product(a, b, NN, count)


def mm_nt(a, b):
    return product(a, b, NT)


def sigmoid(x):
    return 1.0 / (1.0 + jnp.exp(-x))


def same_head(width):
    i = lax.broadcasted_iota(jnp.int32, (LANES, LANES), 0) // width
    j = lax.broadcasted_iota(jnp.int32, (LANES, LANES), 1) // width
    return (i == j).astype(jnp.float32).astype(jnp.bfloat16)


def pair_up(a, b):
    zero = jnp.zeros_like(a)
    return jnp.concatenate(
        [jnp.concatenate([a, zero], axis=1), jnp.concatenate([zero, b], axis=1)], axis=0
    )


def unit_inverses(strict_parts, rows, cols):
    size = strict_parts[0].shape[0]
    pairs = [strict_parts[i : i + 2] for i in range(0, len(strict_parts), 2)]
    eye = (rows == cols).astype(jnp.float32)
    inverses = None
    half = 1
    while half < size:
        off = (rows // (2 * half) == cols // (2 * half)) & (rows // half != cols // half)
        parts = [[jnp.where(off, s, 0.0) for s in pair] for pair in pairs]
        if half == 1:
            inverses = [jnp.concatenate([eye + p for p in pair], axis=1) for pair in parts]
        else:
            middles = [
                product_of(split(inverse), [pair_up(*x) for x in zip(*(split(p) for p in pair))])
                for inverse, pair in zip(inverses, parts)
            ]
            inverses = [
                inverse
                + product_of(
                    split(middle),
                    [pair_up(x[:, :size], x[:, size:]) for x in split(inverse)],
                )
                for inverse, middle in zip(inverses, middles)
            ]
        half *= 2
    return [inverse[:, i * size : (i + 1) * size] for inverse in inverses for i in range(2)]


def product_of(left, right, dims=NN):
    total = None
    for i, p in enumerate(left):
        for j, r in enumerate(right):
            if i + j < 2:
                term = lax.dot_general(p, r, dims, preferred_element_type=jnp.float32)
                total = term if total is None else total + term
    return total


def local_units(widths, tokens):
    T = tokens[0][0].shape[0]
    rows = lax.broadcasted_iota(jnp.int32, (T, T), 0)
    cols = lax.broadcasted_iota(jnp.int32, (T, T), 1)
    inclusive = rows >= cols
    strict = rows > cols
    running = inclusive.astype(jnp.float32).astype(jnp.bfloat16)
    eye = lax.broadcasted_iota(jnp.int32, (LANES, LANES), 0) == lax.broadcasted_iota(
        jnp.int32, (LANES, LANES), 1
    )
    decays = [t[5] - jnp.exp(jnp.float32(-0.5)) * sigmoid(t[3].astype(jnp.float32)) for t in tokens]
    cumulatives = [mm(running, d, 3) for d in decays]
    heads, units = [], []
    for width, (q, k, v, fade, speed, extra), log_decay, cumulative in zip(
        widths, tokens, decays, cumulatives
    ):
        q, k = q.astype(jnp.float32), k.astype(jnp.float32)
        removal = k * lax.rsqrt(mm(k * k, same_head(width)) + key_epsilon)
        left = -removal
        right = sigmoid(speed.astype(jnp.float32)) * removal
        middle = cumulative[T // 2 : T // 2 + 1, :]
        final = cumulative[T - 1 : T, :]
        forward = jnp.exp(cumulative - middle)
        backward = jnp.exp(middle - cumulative)
        tail = jnp.exp(final - cumulative)
        queries = split(jnp.concatenate([left * jnp.exp(-log_decay) * forward, q * forward], axis=0))
        sources = split(jnp.concatenate([right * backward, k * backward], axis=0))
        start_target = left * jnp.exp(cumulative - log_decay)
        right_tail = split(right * tail)
        key_tail = split(k * tail)
        units.append([
            jnp.zeros((T, LANES), jnp.float32),
            q * jnp.exp(cumulative),
            jnp.where(eye, jnp.exp(final), 0.0),
            jnp.zeros((LANES, LANES), jnp.float32),
        ])
        lane = lax.broadcasted_iota(jnp.int32, (1, LANES), 1) // width
        for head in range(LANES // width):
            if width == LANES:
                pick = lambda a: a
            else:
                pick = lambda a, only=lane == head: jnp.where(only, a, jnp.zeros_like(a))
            heads.append((
                len(units) - 1, pick(v), pick(start_target), [pick(x) for x in right_tail],
                [pick(x) for x in key_tail],
                product_of([pick(x) for x in queries], sources, NT),
            ))
    inverses = unit_inverses(
        [jnp.where(strict, h[5][:T, :T], 0.0) for h in heads], rows, cols
    )
    for (u, value, target, head_right, head_key, pairs), inverse in zip(heads, inverses):
        remove_key = jnp.where(strict, pairs[:T, T:], 0.0)
        read_remove = jnp.where(inclusive, pairs[T:, :T], 0.0)
        read_key = jnp.where(inclusive, pairs[T:, T:], 0.0)
        both = mm(inverse, jnp.concatenate([mm(remove_key, value), target], axis=1))
        reads = mm(read_remove, both)
        moved = product_of(split(both), head_right, TN)
        units[u][0] = units[u][0] + reads[:, :LANES] + mm(read_key, value)
        units[u][1] = units[u][1] + reads[:, LANES:]
        units[u][2] = units[u][2] + moved[LANES:]
        units[u][3] = units[u][3] + moved[:LANES] + product_of([value], head_key, TN)
    return units


def finish_unit(width, read, q, k, v, gain, own, gate):
    ones = same_head(width)
    mean = mm(read, ones) / width
    centered = read - mean
    variance = mm(centered * centered, ones) / width
    normed = centered * lax.rsqrt(variance + head_epsilon) * gain
    diagonal = mm(q * k * own, ones) * v
    return ((normed + diagonal) * gate).astype(jnp.bfloat16)


def members_of(n_sp):
    best = 1
    for count in range(1, n_sp + 1):
        if n_sp % count == 0 and count * count <= 2 * n_sp:
            best = count
    return best


def layer_kernel(
    n_sp, n_tp, widths, q_ref, k_ref, v_ref, f_ref, a_ref, e_ref, g_ref, gain_ref, own_ref,
    residual_ref, scale_ref, project_hbm, gate_hbm, up_hbm, down_hbm,
    out_ref,
    local_ref, read_ref, near, total_move, total_add, chain_in, chain_out, mixed_ref, project,
    total, wide, tall, pair_send, pair_got, term_send, term_got, hidden, active, summed,
    low_send, low_got, high_send, high_got, line_send, line_got,
    project_sem, keep_sem, out_sem, in_sem, pass_out, pass_in,
    near_out, near_in, chain_sem_out, chain_sem_in, pair_out, pair_in, term_out, term_in,
    row_out, row_in, up_out, up_in, side_out, side_in,
    low_out, low_in, high_out, high_in, line_out, line_in, mate_out,
):
    F = members_of(n_sp)
    T = n_sp // F
    LO = 2 if n_tp % 2 == 0 else 1
    HI = n_tp // LO
    me = lax.axis_index("sp")
    t = lax.axis_index("tp")
    m, g = me // T, me % T
    hi, lo = t // LO, t % LO
    tokens = q_ref.shape[1]
    rows = gate_hbm.shape[0]
    depth = hidden.shape[1]
    own_cols = depth // n_tp
    down_cols = down_hbm.shape[1]
    base, extra = divmod(gate_hbm.shape[1] // LANES, F)
    parts = 2 if extra else 1

    def member(d):
        return lax.rem(m + d + F, F)

    def other(e):
        return lax.rem(g + e + T, T)

    def cell(h, l):
        return lax.rem(hi + h + HI, HI) * LO + lax.rem(lo + l + LO, LO)

    def remote(src, dst, send, recv, sp, tp):
        return pltpu.make_async_remote_copy(
            src_ref=src, dst_ref=dst, send_sem=send, recv_sem=recv,
            device_id=(sp, tp), device_id_type=MESH,
        )

    barrier = pltpu.get_barrier_semaphore()

    def greet(sp, tp):
        pl.semaphore_signal(barrier, inc=1, device_id=(sp, tp), device_id_type=MESH)

    for d in range(1, F):
        greet(member(d) * T + g, t)
    for e in range(1, T):
        greet(m * T + other(e), t)
    for d in range(1, n_tp):
        greet(me, lax.rem(t + d, n_tp))
    project_copy = pltpu.make_async_copy(project_hbm, project, project_sem)
    project_copy.start()
    pl.semaphore_wait(barrier, F + T + n_tp - 3)

    def more(dest):
        return jnp.where(t % 2 == 0, dest < extra, dest >= F - extra)

    def source(w, part, dest):
        before = jnp.where(t % 2 == 0, jnp.minimum(dest, extra), jnp.maximum(dest - F + extra, 0))
        tile = dest * base + before + (base if part else 0)
        at = pl.ds(pl.multiple_of(tile * LANES, LANES), LANES if part else base * LANES)
        return down_hbm.at[at, :] if w == 2 else (gate_hbm, up_hbm)[w].at[:, at]

    def landing(w, part, s):
        at = pl.ds(base * LANES if part else 0, LANES if part else base * LANES)
        if w == 2:
            return tall.at[s, at, :]
        return wide.at[w, pl.ds(pl.multiple_of(s * rows, rows), rows), at]

    def guarded(part, dest, action):
        if part:
            pl.when(more(dest))(action)
        else:
            action()

    def give(w, part, d):
        dest = member(d)
        return remote(
            source(w, part, dest), landing(w, part, me), out_sem.at[w, part, d],
            in_sem.at[w, part, d], dest * T + g, t,
        )

    def take(w, part, d):
        return remote(
            source(w, part, m), landing(w, part, member(-d) * T + g), out_sem.at[w, part, d],
            in_sem.at[w, part, d], me, t,
        )

    def hand(w, part, d, e):
        s = member(-d) * T + g
        src = source(w, part, m) if d == 0 else landing(w, part, s)
        return remote(
            src, landing(w, part, s), pass_out.at[w, part, d, e], pass_in.at[w, part, d, e],
            m * T + other(e), t,
        )

    def accept(w, part, d, e):
        s = member(-d) * T + other(-e)
        return remote(
            source(w, part, m), landing(w, part, s), pass_out.at[w, part, d, e],
            pass_in.at[w, part, d, e], me, t,
        )

    def keep(w, part):
        return pltpu.make_async_copy(
            source(w, part, m), landing(w, part, me), keep_sem.at[w, part]
        )

    def open_weight(w):
        for part in range(parts):

            def begin():
                keep(w, part).start()
                for e in range(1, T):
                    hand(w, part, 0, e).start()

            guarded(part, m, begin)

    def send_part(w, part, d, upward):
        dest = member(d)
        chosen = dest > m if upward else dest < m
        if part:
            chosen = chosen & more(dest)
        pl.when(chosen)(lambda: give(w, part, d).start())

    def send_weight(w, upward, chosen_parts):
        for part in chosen_parts:
            for d in range(F - 1, 0, -1) if upward else range(1, F):
                send_part(w, part, d, upward)

    def send_near_first(w, upward, chosen_parts):
        for d in range(1, F) if upward else range(F - 1, 0, -1):
            for part in chosen_parts:
                send_part(w, part, d, upward)

    def relay_weight(w, chosen_parts):
        for part in chosen_parts:
            for d in range(1, F):

                def pass_on():
                    take(w, part, d).wait_recv()
                    for e in range(1, T):
                        hand(w, part, d, e).start()

                guarded(part, m, pass_on)

    def arrived_weight(w):
        for part in range(parts):

            def settle():
                keep(w, part).wait()
                for d in range(F):
                    for e in range(1, T):
                        accept(w, part, d, e).wait_recv()

            guarded(part, m, settle)

    every, first, rest = range(parts), range(1), range(1, parts)
    open_weight(0)
    send_weight(0, True, every)
    send_weight(0, False, every)
    send_weight(1, False, every)
    send_weight(2, False, first)
    if extra:

        @pl.when(jnp.logical_not(more(m)))
        def _():
            tall[:, base * LANES :, :] = jnp.zeros(
                (n_sp, LANES, down_cols), jnp.bfloat16
            )

    per_group = q_ref.shape[2] // LANES

    def load(ref, group, c):
        return ref[group, :, c * LANES : (c + 1) * LANES].astype(jnp.float32)

    units = [(group, c) for group in range(2) for c in range(per_group)]

    def near_copy(u, e):
        return remote(
            near.at[g, u], near.at[g, u], near_out.at[u, e], near_in.at[u, e],
            m * T + other(e), t,
        )

    def near_take(u, e):
        return remote(
            near.at[other(-e), u], near.at[other(-e), u], near_out.at[u, e],
            near_in.at[u, e], me, t,
        )

    def blocks(group, c):
        lanes = slice(c * LANES, (c + 1) * LANES)
        return [r[group, :, lanes] for r in (q_ref, k_ref, v_ref, f_ref, a_ref, e_ref)]

    local = local_units([widths[group] for group, _ in units], [blocks(*unit) for unit in units])
    for u, (local_out, start_read, transit, added) in enumerate(local):
        local_ref[u] = local_out
        read_ref[u] = start_read
        near[g, u, 0] = transit.astype(jnp.bfloat16)
        near[g, u, 1] = added.astype(jnp.bfloat16)
    for u in range(len(units)):
        for e in range(1, T):
            near_copy(u, e).start()

    @pl.when(m == 0)
    def _():
        chain_in[...] = jnp.zeros_like(chain_in)

    open_weight(1)
    open_weight(2)

    def chain_copy(u):
        return remote(
            chain_out.at[u], chain_in.at[u], chain_sem_out.at[u], chain_sem_in.at[u],
            member(1) * T + g, t,
        )

    for u in range(len(units)):
        for e in range(1, T):
            near_take(u, e).wait_recv()
        move, add = near[0, u, 0], near[0, u, 1].astype(jnp.float32)
        for other_g in range(1, T):
            step = near[other_g, u, 0]
            add = mm(add, step) + near[other_g, u, 1].astype(jnp.float32)
            move = mm(move, step).astype(jnp.bfloat16)
        total_move[u] = move
        total_add[u] = add
    for u in range(len(units)):

        @pl.when(m > 0)
        def _():
            chain_copy(u).wait_recv()

        following = mm(chain_in[u], total_move[u]) + total_add[u]
        chain_out[u] = following.astype(jnp.bfloat16)

        @pl.when(m < F - 1)
        def _():
            chain_copy(u).start()

    send_near_first(1, True, every)
    send_near_first(2, True, first)
    relay_weight(0, range(parts))

    def fold(other_g, states):
        return tuple(
            mm(s, near[other_g, u, 0]) + near[other_g, u, 1].astype(jnp.float32)
            for u, s in enumerate(states)
        )

    states = lax.fori_loop(
        0, g, fold, tuple(chain_in[u].astype(jnp.float32) for u in range(len(units)))
    )
    for u, (group, c) in enumerate(units):
        lanes = slice(c * LANES, (c + 1) * LANES)
        read = local_ref[u] + mm_nt(read_ref[u], states[u])
        mixed_ref[:, u * LANES : (u + 1) * LANES] = finish_unit(
            widths[group], read, load(q_ref, group, c), load(k_ref, group, c),
            load(v_ref, group, c), gain_ref[group : group + 1, lanes],
            own_ref[group : group + 1, lanes], load(g_ref, group, c),
        )

    project_copy.wait()
    mixed = mixed_ref[...]

    def columns(at):
        return pl.ds(pl.multiple_of(at * own_cols, own_cols), own_cols)

    def term(at):
        return jnp.dot(mixed, project[:, columns(at)], preferred_element_type=jnp.float32)

    def pair_copy(h, l):
        return remote(
            pair_send.at[h, l], pair_got.at[h, l], pair_out.at[h, l], pair_in.at[h, l],
            me, cell(0, l),
        )

    def term_copy(h):
        return remote(
            term_send.at[h], term_got.at[h], term_out.at[h], term_in.at[h], me, cell(h, 0)
        )

    far = list(range(1, HI)) + [0]
    for h in far:
        for l in range(1, LO):
            pair_send[h, l] = term(cell(h, l)).astype(jnp.bfloat16)
            pair_copy(h, l).start()
    for h in far:
        branch = term(cell(h, 0))
        for l in range(1, LO):
            pair_copy(h, l).wait_recv()
            branch = branch + pair_got[h, l].astype(jnp.float32)
        if h:
            term_send[h] = branch.astype(jnp.bfloat16)
            term_copy(h).start()
    for h in range(1, HI):
        term_copy(h).wait_recv()
        branch = branch + term_got[h].astype(jnp.float32)

    def positions(at):
        return pl.ds(pl.multiple_of(at * tokens, tokens), tokens)

    own_state = (residual_ref[:, columns(t)].astype(jnp.float32) + branch).astype(jnp.bfloat16)
    hidden[positions(m), columns(t)] = own_state

    def block(a, at):
        return hidden.at[positions(a), columns(at)]

    def row_copy(a, d):
        return remote(
            block(a, t), block(a, t), row_out.at[d], row_in.at[a], member(d) * T + g, t
        )

    def nearer(b, a):
        return (b // 2 == a // 2) | ((a > b) == (b % 2 == 1)) | (F % 2 == 1)

    def mate_copy(a):
        return remote(
            block(a, t), block(a, t), mate_out.at[a], row_in.at[a],
            (m + 1 - 2 * (m % 2)) * T + g, t,
        )

    def hands_on(a):
        return nearer(m, a) & (a // 2 != m // 2) & (F % 2 == 0)

    def up_copy(a, h):
        return remote(block(a, t), block(a, t), up_out.at[a, h], up_in.at[a, h], me, cell(h, 0))

    def up_take(a, h):
        at = block(a, cell(-h, 0))
        return remote(at, at, up_out.at[a, h], up_in.at[a, h], me, t)

    def side_copy(a, h, l):
        at = block(a, cell(-h, 0))
        return remote(at, at, side_out.at[a, h, l], side_in.at[a, h, l], me, cell(0, l))

    def side_take(a, h, l):
        at = block(a, cell(-h, -l))
        return remote(at, at, side_out.at[a, h, l], side_in.at[a, h, l], me, t)

    def spread(a):
        for h in range(1, HI):
            up_copy(a, h).start()
        for l in range(1, LO):
            side_copy(a, 0, l).start()

    width = wide.shape[2]
    have = (base + more(m).astype(jnp.int32)) * LANES if extra else width

    def activate(a):
        state = hidden[positions(a), :].astype(jnp.float32)
        power = jnp.sum(state * state, axis=1, keepdims=True) / depth
        normed = (state * lax.rsqrt(power + norm_epsilon) * scale_ref[...]).astype(jnp.bfloat16)
        gate_pre = jnp.dot(normed, wide[0], preferred_element_type=jnp.float32)
        up_pre = jnp.dot(normed, wide[1], preferred_element_type=jnp.float32)
        value = gate_pre / (1.0 + jnp.exp(-gate_pre)) * up_pre
        if extra:
            lane = lax.broadcasted_iota(jnp.int32, (1, width), 1)
            value = jnp.where(lane < have, value, 0.0)
        active[positions(a), :] = value.astype(jnp.bfloat16)

    for d in range(1, F):
        pl.when((m + d < F) & nearer(member(d), m))(lambda: row_copy(m, d).start())
    for d in range(1, F):
        pl.when((m + d >= F) & nearer(member(d), m))(lambda: row_copy(m, d).start())
    spread(m)
    send_weight(2, True, rest)
    send_weight(2, False, rest)
    relay_weight(1, range(parts))

    def turn(k):
        return jnp.where(k == 0, m, k - 1 + (k - 1 >= m).astype(jnp.int32))

    def target(k):
        rising = k + (k >= m).astype(jnp.int32)
        falling = F - 1 - k - (F - 1 - k <= m).astype(jnp.int32)
        return jnp.where(k == F - 1, m, jnp.where(2 * m >= F, rising, falling))

    def low_copy(k, h, l):
        return remote(
            low_send.at[k, h, l], low_got.at[k, h, l], low_out.at[k, h, l],
            low_in.at[k, h, l], me, cell(0, l),
        )

    def high_copy(k, h):
        return remote(
            high_send.at[k, h], high_got.at[k, h], high_out.at[k, h], high_in.at[k, h],
            me, cell(h, 0),
        )

    def line_copy(k):
        return remote(
            line_send.at[k], line_got.at[m], line_out.at[k], line_in.at[m], target(k) * T + g, t
        )

    def line_take(a):
        return remote(line_send.at[0], line_got.at[a], line_out.at[0], line_in.at[a], me, t)

    def across(k):
        for h in range(1, HI):
            up_take(turn(k), h).wait_recv()
            for l in range(1, LO):
                side_copy(turn(k), h, l).start()

    def gathered(k):
        for h in range(HI):
            for l in range(1, LO):
                side_take(turn(k), h, l).wait_recv()
        activate(turn(k))

    def contract(k):
        here = positions(target(k))
        units_here = active[here, :]
        for s in range(n_sp):
            summed[here, s * down_cols : (s + 1) * down_cols] = jnp.dot(
                units_here, tall[s], preferred_element_type=jnp.float32
            )
        for h in far:
            for l in range(1, LO):
                low_send[k, h, l] = summed[here, columns(cell(h, l))].astype(jnp.bfloat16)
                low_copy(k, h, l).start()

    def two_cores(k, h):
        value = summed[positions(target(k)), columns(cell(h, 0))]
        for l in range(1, LO):
            value = value + low_got[k, h, l].astype(jnp.float32)
        return value

    def halve(k):
        for h in range(HI):
            for l in range(1, LO):
                low_copy(k, h, l).wait_recv()
        for h in range(1, HI):
            high_send[k, h] = two_cores(k, h).astype(jnp.bfloat16)
            high_copy(k, h).start()

    def whole(k):
        value = two_cores(k, 0)
        for h in range(1, HI):
            high_copy(k, h).wait_recv()
            value = value + high_got[k, h].astype(jnp.float32)
        return value

    across(0)

    @pl.loop(1, F + 1)
    def _(i):
        @pl.when(i < F)
        def _():
            row_copy(turn(i), 0).wait_recv()
            pl.when(hands_on(turn(i)))(lambda: mate_copy(turn(i)).start())
            spread(turn(i))

            @pl.when(i == 1)
            def _():
                relay_weight(2, first)

            @pl.when(i == F - 1)
            def _():
                relay_weight(2, rest)

        @pl.when(i >= 2)
        def _():
            across(i - 1)

        @pl.when(i == 2)
        def _():
            arrived_weight(0)
            arrived_weight(1)

        @pl.when(i >= 3)
        def _():
            gathered(i - 3)

    @pl.loop(max(F - 2, 0), F)
    def _(k):
        gathered(k)

    arrived_weight(2)

    @pl.loop(0, F)
    def _(k):
        contract(k)

    @pl.loop(0, F)
    def _(k):
        halve(k)

    @pl.loop(0, F - 1)
    def _(k):
        line_send[k] = whole(k).astype(jnp.bfloat16)
        line_copy(k).start()

    total[...] = hidden[positions(m), columns(t)].astype(jnp.float32) + whole(F - 1)

    @pl.loop(0, F)
    def _(a):
        @pl.when(a != m)
        def _():
            line_take(a).wait_recv()
            total[...] += line_got[a].astype(jnp.float32)

    out_ref[...] = total[...].astype(jnp.bfloat16)

    for w in range(3):
        for part in range(parts):
            for d in range(1, F):
                guarded(part, member(d), lambda: give(w, part, d).wait_send())

            def passed():
                for d in range(F):
                    for e in range(1, T):
                        hand(w, part, d, e).wait_send()

            guarded(part, m, passed)
    for u in range(len(units)):
        for e in range(1, T):
            near_copy(u, e).wait_send()

    @pl.when(m < F - 1)
    def _():
        for u in range(len(units)):
            chain_copy(u).wait_send()

    for h in range(HI):
        if h:
            term_copy(h).wait_send()
        for l in range(1, LO):
            pair_copy(h, l).wait_send()
    for d in range(F):
        if d:
            pl.when(nearer(member(d), m))(lambda: row_copy(m, d).wait_send())
            line_copy(d - 1).wait_send()
        pl.when(hands_on(d))(lambda: mate_copy(d).wait_send())
        for h in range(HI):
            if h:
                up_copy(d, h).wait_send()
                high_copy(d, h).wait_send()
            for l in range(1, LO):
                side_copy(d, h, l).wait_send()
                low_copy(d, h, l).wait_send()


def layer(n_sp, n_tp, q, k, v, f, a, e, g, gain, own, residual, scale, project, gate, up, down):
    tokens, channels = q.shape[1], q.shape[2]
    units = 2 * channels // LANES
    depth = residual.shape[1]
    cols = depth // n_tp
    F = members_of(n_sp)
    T = n_sp // F
    LO = 2 if n_tp % 2 == 0 else 1
    HI = n_tp // LO
    width = -(-(gate.shape[1] // LANES) // F) * LANES
    vmem = pl.BlockSpec(memory_space=pltpu.VMEM)
    hbm = pl.BlockSpec(memory_space=pl.ANY)
    bf16, f32 = jnp.bfloat16, jnp.float32
    sem = pltpu.SemaphoreType.DMA
    scratch = [
        pltpu.VMEM((units, tokens, LANES), f32),
        pltpu.VMEM((units, tokens, LANES), f32),
        pltpu.VMEM((T, units, 2, LANES, LANES), bf16),
        pltpu.VMEM((units, LANES, LANES), bf16),
        pltpu.VMEM((units, LANES, LANES), f32),
        pltpu.VMEM((units, LANES, LANES), bf16),
        pltpu.VMEM((units, LANES, LANES), bf16),
        pltpu.VMEM((tokens, units * LANES), bf16),
        pltpu.VMEM(project.shape, bf16),
        pltpu.VMEM((tokens, cols), f32),
        pltpu.VMEM((2, depth, width), bf16),
        pltpu.VMEM((n_sp, width, down.shape[1]), bf16),
        pltpu.VMEM((HI, LO, tokens, cols), bf16),
        pltpu.VMEM((HI, LO, tokens, cols), bf16),
        pltpu.VMEM((HI, tokens, cols), bf16),
        pltpu.VMEM((HI, tokens, cols), bf16),
        pltpu.VMEM((F * tokens, depth), bf16),
        pltpu.VMEM((F * tokens, width), bf16),
        pltpu.VMEM((F * tokens, depth), f32),
        pltpu.VMEM((F, HI, LO, tokens, cols), bf16),
        pltpu.VMEM((F, HI, LO, tokens, cols), bf16),
        pltpu.VMEM((F, HI, tokens, cols), bf16),
        pltpu.VMEM((F, HI, tokens, cols), bf16),
        pltpu.VMEM((F, tokens, cols), bf16),
        pltpu.VMEM((F, tokens, cols), bf16),
        sem, sem((3, 2)),
    ]
    for shape in (
        (3, 2, F), (3, 2, F, T), (units, T), (units,), (HI, LO), (HI,), (F,), (F, HI), (F, HI, LO),
        (F, HI, LO), (F, HI), (F,),
    ):
        scratch += [sem(shape), sem(shape)]
    scratch.append(sem((F,)))
    return pl.pallas_call(
        functools.partial(layer_kernel, n_sp, n_tp, (DS, DL)),
        out_shape=jax.ShapeDtypeStruct((tokens, cols), bf16),
        in_specs=[vmem] * 11 + [hbm] * 4,
        out_specs=vmem,
        scratch_shapes=scratch,
        compiler_params=pltpu.CompilerParams(
            collective_id=0, has_side_effects=True, vmem_limit_bytes=60 * 2**20
        ),
        name="layer",
    )(q, k, v, f, a, e, g, gain, own, residual, scale, project, gate, up, down)


def on_device(
    stratum_source_matrix,
    acceptance_query,
    cluster_lookup_matrix,
    cluster_payload_matrix,
    fading_logit,
    adaptation_speed_logit,
    additional_fading_exponent,
    result_switch_pair,
    attender_scaling_factor,
    present_item_factor,
    final_mapping_matrix,
    perceptron_scaling_factor,
    switching_matrix,
    widening_matrix,
    shrinking_matrix,
):
    return layer(
        lax.axis_size("sp"),
        lax.axis_size("tp"),
        acceptance_query,
        cluster_lookup_matrix,
        cluster_payload_matrix,
        fading_logit,
        adaptation_speed_logit,
        additional_fading_exponent,
        result_switch_pair,
        attender_scaling_factor,
        present_item_factor,
        stratum_source_matrix,
        perceptron_scaling_factor.reshape(1, -1),
        final_mapping_matrix.reshape(-1, final_mapping_matrix.shape[2]),
        switching_matrix,
        widening_matrix,
        shrinking_matrix,
    )


def solution(mesh):
    tokens = P(None, "sp", "tp")
    in_specs = (
        P("sp", None), tokens, tokens, tokens, tokens, tokens, tokens, tokens,
        P(None, "tp"), P(None, "tp"), P(None, "tp", None), P(),
        P("sp", "tp"), P("sp", "tp"), P("tp", "sp"),
    )
    return jax.shard_map(
        on_device, mesh=mesh, in_specs=in_specs, out_specs=P("sp", "tp"), check_vma=False
    )
```

```python
import functools

import jax
import jax.numpy as jnp
from jax import lax
from jax.experimental import pallas as pl
from jax.experimental.pallas import tpu as pltpu
from jax.sharding import PartitionSpec as P

DS = 64
DL = 128
LANES = 128
MESH = pl.DeviceIdType.MESH

norm_epsilon = 1e-06
head_epsilon = 0.00064
key_epsilon = 1e-06


NN = (((1,), (0,)), ((), ()))
NT = (((1,), (1,)), ((), ()))
TN = (((0,), (0,)), ((), ()))


def split(x, count=2):
    if x.dtype == jnp.bfloat16:
        return [x]
    parts = []
    for _ in range(count - 1):
        high = x.astype(jnp.bfloat16)
        parts.append(high)
        x = x - high.astype(jnp.float32)
    return parts + [x.astype(jnp.bfloat16)]


def product(a, b, dims, count=2):
    total = None
    for i, p in enumerate(split(a, count)):
        for j, r in enumerate(split(b, count)):
            if i + j < count:
                term = lax.dot_general(p, r, dims, preferred_element_type=jnp.float32)
                total = term if total is None else total + term
    return total


def mm(a, b, count=2):
    return product(a, b, NN, count)


def mm_nt(a, b):
    return product(a, b, NT)


def sigmoid(x):
    return 1.0 / (1.0 + jnp.exp(-x))


def same_head(width):
    i = lax.broadcasted_iota(jnp.int32, (LANES, LANES), 0) // width
    j = lax.broadcasted_iota(jnp.int32, (LANES, LANES), 1) // width
    return (i == j).astype(jnp.float32).astype(jnp.bfloat16)


def pair_up(a, b):
    zero = jnp.zeros_like(a)
    return jnp.concatenate(
        [jnp.concatenate([a, zero], axis=1), jnp.concatenate([zero, b], axis=1)], axis=0
    )


def unit_inverses(strict_parts, rows, cols):
    size = strict_parts[0].shape[0]
    pairs = [strict_parts[i : i + 2] for i in range(0, len(strict_parts), 2)]
    eye = (rows == cols).astype(jnp.float32)
    inverses = None
    half = 1
    while half < size:
        off = (rows // (2 * half) == cols // (2 * half)) & (rows // half != cols // half)
        parts = [[jnp.where(off, s, 0.0) for s in pair] for pair in pairs]
        if half == 1:
            inverses = [jnp.concatenate([eye + p for p in pair], axis=1) for pair in parts]
        else:
            middles = [
                product_of(split(inverse), [pair_up(*x) for x in zip(*(split(p) for p in pair))])
                for inverse, pair in zip(inverses, parts)
            ]
            inverses = [
                inverse
                + product_of(
                    split(middle),
                    [pair_up(x[:, :size], x[:, size:]) for x in split(inverse)],
                )
                for inverse, middle in zip(inverses, middles)
            ]
        half *= 2
    return [inverse[:, i * size : (i + 1) * size] for inverse in inverses for i in range(2)]


def product_of(left, right, dims=NN):
    total = None
    for i, p in enumerate(left):
        for j, r in enumerate(right):
            if i + j < 2:
                term = lax.dot_general(p, r, dims, preferred_element_type=jnp.float32)
                total = term if total is None else total + term
    return total


def local_units(widths, tokens):
    T = tokens[0][0].shape[0]
    rows = lax.broadcasted_iota(jnp.int32, (T, T), 0)
    cols = lax.broadcasted_iota(jnp.int32, (T, T), 1)
    inclusive = rows >= cols
    strict = rows > cols
    running = inclusive.astype(jnp.float32).astype(jnp.bfloat16)
    eye = lax.broadcasted_iota(jnp.int32, (LANES, LANES), 0) == lax.broadcasted_iota(
        jnp.int32, (LANES, LANES), 1
    )
    decays = [t[5] - jnp.exp(jnp.float32(-0.5)) * sigmoid(t[3].astype(jnp.float32)) for t in tokens]
    cumulatives = [mm(running, d, 3) for d in decays]
    heads, units = [], []
    for width, (q, k, v, fade, speed, extra), log_decay, cumulative in zip(
        widths, tokens, decays, cumulatives
    ):
        q, k = q.astype(jnp.float32), k.astype(jnp.float32)
        removal = k * lax.rsqrt(mm(k * k, same_head(width)) + key_epsilon)
        left = -removal
        right = sigmoid(speed.astype(jnp.float32)) * removal
        middle = cumulative[T // 2 : T // 2 + 1, :]
        final = cumulative[T - 1 : T, :]
        forward = jnp.exp(cumulative - middle)
        backward = jnp.exp(middle - cumulative)
        tail = jnp.exp(final - cumulative)
        queries = split(jnp.concatenate([left * jnp.exp(-log_decay) * forward, q * forward], axis=0))
        sources = split(jnp.concatenate([right * backward, k * backward], axis=0))
        start_target = left * jnp.exp(cumulative - log_decay)
        right_tail = split(right * tail)
        key_tail = split(k * tail)
        units.append([
            jnp.zeros((T, LANES), jnp.float32),
            q * jnp.exp(cumulative),
            jnp.where(eye, jnp.exp(final), 0.0),
            jnp.zeros((LANES, LANES), jnp.float32),
        ])
        lane = lax.broadcasted_iota(jnp.int32, (1, LANES), 1) // width
        for head in range(LANES // width):
            if width == LANES:
                pick = lambda a: a
            else:
                pick = lambda a, only=lane == head: jnp.where(only, a, jnp.zeros_like(a))
            heads.append((
                len(units) - 1, pick(v), pick(start_target), [pick(x) for x in right_tail],
                [pick(x) for x in key_tail],
                product_of([pick(x) for x in queries], sources, NT),
            ))
    inverses = unit_inverses(
        [jnp.where(strict, h[5][:T, :T], 0.0) for h in heads], rows, cols
    )
    for (u, value, target, head_right, head_key, pairs), inverse in zip(heads, inverses):
        remove_key = jnp.where(strict, pairs[:T, T:], 0.0)
        read_remove = jnp.where(inclusive, pairs[T:, :T], 0.0)
        read_key = jnp.where(inclusive, pairs[T:, T:], 0.0)
        both = mm(inverse, jnp.concatenate([mm(remove_key, value), target], axis=1))
        reads = mm(read_remove, both)
        moved = product_of(split(both), head_right, TN)
        units[u][0] = units[u][0] + reads[:, :LANES] + mm(read_key, value)
        units[u][1] = units[u][1] + reads[:, LANES:]
        units[u][2] = units[u][2] + moved[LANES:]
        units[u][3] = units[u][3] + moved[:LANES] + product_of([value], head_key, TN)
    return units


def finish_unit(width, read, q, k, v, gain, own, gate):
    ones = same_head(width)
    mean = mm(read, ones) / width
    centered = read - mean
    variance = mm(centered * centered, ones) / width
    normed = centered * lax.rsqrt(variance + head_epsilon) * gain
    diagonal = mm(q * k * own, ones) * v
    return ((normed + diagonal) * gate).astype(jnp.bfloat16)


def members_of(n_sp):
    best = 1
    for count in range(1, n_sp + 1):
        if n_sp % count == 0 and count * count <= 2 * n_sp:
            best = count
    return best


def layer_kernel(
    n_sp, n_tp, widths, q_ref, k_ref, v_ref, f_ref, a_ref, e_ref, g_ref, gain_ref, own_ref,
    residual_ref, scale_ref, project_hbm, gate_hbm, up_hbm, down_hbm,
    out_ref,
    local_ref, read_ref, near, total_move, total_add, chain_in, chain_out, mixed_ref, project,
    total, wide, tall, pair_send, pair_got, term_send, term_got, hidden, active, summed,
    low_send, low_got, high_send, high_got, line_send, line_got,
    project_sem, keep_sem, out_sem, in_sem, pass_out, pass_in,
    near_out, near_in, chain_sem_out, chain_sem_in, pair_out, pair_in, term_out, term_in,
    row_out, row_in, up_out, up_in, side_out, side_in,
    low_out, low_in, high_out, high_in, line_out, line_in, mate_out,
):
    F = members_of(n_sp)
    T = n_sp // F
    LO = 2 if n_tp % 2 == 0 else 1
    HI = n_tp // LO
    me = lax.axis_index("sp")
    t = lax.axis_index("tp")
    m, g = me // T, me % T
    hi, lo = t // LO, t % LO
    tokens = q_ref.shape[1]
    rows = gate_hbm.shape[0]
    depth = hidden.shape[1]
    own_cols = depth // n_tp
    down_cols = down_hbm.shape[1]
    base, extra = divmod(gate_hbm.shape[1] // LANES, F)
    parts = 2 if extra else 1

    def member(d):
        return lax.rem(m + d + F, F)

    def other(e):
        return lax.rem(g + e + T, T)

    def cell(h, l):
        return lax.rem(hi + h + HI, HI) * LO + lax.rem(lo + l + LO, LO)

    def remote(src, dst, send, recv, sp, tp):
        return pltpu.make_async_remote_copy(
            src_ref=src, dst_ref=dst, send_sem=send, recv_sem=recv,
            device_id=(sp, tp), device_id_type=MESH,
        )

    barrier = pltpu.get_barrier_semaphore()

    def greet(sp, tp):
        pl.semaphore_signal(barrier, inc=1, device_id=(sp, tp), device_id_type=MESH)

    for d in range(1, F):
        greet(member(d) * T + g, t)
    for e in range(1, T):
        greet(m * T + other(e), t)
    for d in range(1, n_tp):
        greet(me, lax.rem(t + d, n_tp))
    project_copy = pltpu.make_async_copy(project_hbm, project, project_sem)
    project_copy.start()
    pl.semaphore_wait(barrier, F + T + n_tp - 3)

    def more(dest):
        return jnp.where(t % 2 == 0, dest < extra, dest >= F - extra)

    def source(w, part, dest):
        before = jnp.where(t % 2 == 0, jnp.minimum(dest, extra), jnp.maximum(dest - F + extra, 0))
        tile = dest * base + before + (base if part else 0)
        at = pl.ds(pl.multiple_of(tile * LANES, LANES), LANES if part else base * LANES)
        return down_hbm.at[at, :] if w == 2 else (gate_hbm, up_hbm)[w].at[:, at]

    def landing(w, part, s):
        at = pl.ds(base * LANES if part else 0, LANES if part else base * LANES)
        if w == 2:
            return tall.at[s, at, :]
        return wide.at[w, pl.ds(pl.multiple_of(s * rows, rows), rows), at]

    def guarded(part, dest, action):
        if part:
            pl.when(more(dest))(action)
        else:
            action()

    def give(w, part, d):
        dest = member(d)
        return remote(
            source(w, part, dest), landing(w, part, me), out_sem.at[w, part, d],
            in_sem.at[w, part, d], dest * T + g, t,
        )

    def take(w, part, d):
        return remote(
            source(w, part, m), landing(w, part, member(-d) * T + g), out_sem.at[w, part, d],
            in_sem.at[w, part, d], me, t,
        )

    def hand(w, part, d, e):
        s = member(-d) * T + g
        src = source(w, part, m) if d == 0 else landing(w, part, s)
        return remote(
            src, landing(w, part, s), pass_out.at[w, part, d, e], pass_in.at[w, part, d, e],
            m * T + other(e), t,
        )

    def accept(w, part, d, e):
        s = member(-d) * T + other(-e)
        return remote(
            source(w, part, m), landing(w, part, s), pass_out.at[w, part, d, e],
            pass_in.at[w, part, d, e], me, t,
        )

    def keep(w, part):
        return pltpu.make_async_copy(
            source(w, part, m), landing(w, part, me), keep_sem.at[w, part]
        )

    def open_weight(w):
        for part in range(parts):

            def begin():
                keep(w, part).start()
                for e in range(1, T):
                    hand(w, part, 0, e).start()

            guarded(part, m, begin)

    def send_part(w, part, d, upward):
        dest = member(d)
        chosen = dest > m if upward else dest < m
        if part:
            chosen = chosen & more(dest)
        pl.when(chosen)(lambda: give(w, part, d).start())

    def send_weight(w, upward, chosen_parts):
        for part in chosen_parts:
            for d in range(F - 1, 0, -1) if upward else range(1, F):
                send_part(w, part, d, upward)

    def send_near_first(w, upward, chosen_parts):
        for d in range(1, F) if upward else range(F - 1, 0, -1):
            for part in chosen_parts:
                send_part(w, part, d, upward)

    def relay_weight(w, chosen_parts):
        for part in chosen_parts:
            for d in range(1, F):

                def pass_on():
                    take(w, part, d).wait_recv()
                    for e in range(1, T):
                        hand(w, part, d, e).start()

                guarded(part, m, pass_on)

    def arrived_weight(w):
        for part in range(parts):

            def settle():
                keep(w, part).wait()
                for d in range(F):
                    for e in range(1, T):
                        accept(w, part, d, e).wait_recv()

            guarded(part, m, settle)

    every, first, rest = range(parts), range(1), range(1, parts)
    open_weight(0)
    send_weight(0, True, every)
    send_weight(0, False, every)
    send_weight(1, False, every)
    send_weight(2, False, first)
    if extra:

        @pl.when(jnp.logical_not(more(m)))
        def _():
            tall[:, base * LANES :, :] = jnp.zeros(
                (n_sp, LANES, down_cols), jnp.bfloat16
            )

    per_group = q_ref.shape[2] // LANES

    def load(ref, group, c):
        return ref[group, :, c * LANES : (c + 1) * LANES].astype(jnp.float32)

    units = [(group, c) for group in range(2) for c in range(per_group)]

    def own_rows(u):
        return pl.ds(0, widths[units[u][0]])

    def pack(u, x):
        width = widths[units[u][0]]
        return sum(x[at : at + width] for at in range(0, LANES, width)).astype(jnp.bfloat16)

    def unpack(u, x):
        width = widths[units[u][0]]
        if width == LANES:
            return x
        return jnp.concatenate([x] * (LANES // width), axis=0) * same_head(width)

    def near_state(source_g, u, i):
        return unpack(u, near[source_g, u, i, own_rows(u), :])

    def near_copy(u, e):
        at = near.at[g, u, :, own_rows(u)]
        return remote(
            at, at, near_out.at[u, e], near_in.at[u, e],
            m * T + other(e), t,
        )

    def near_take(u, e):
        at = near.at[other(-e), u, :, own_rows(u)]
        return remote(
            at, at, near_out.at[u, e],
            near_in.at[u, e], me, t,
        )

    def blocks(group, c):
        lanes = slice(c * LANES, (c + 1) * LANES)
        return [r[group, :, lanes] for r in (q_ref, k_ref, v_ref, f_ref, a_ref, e_ref)]

    local = local_units([widths[group] for group, _ in units], [blocks(*unit) for unit in units])
    for u, (local_out, start_read, transit, added) in enumerate(local):
        local_ref[u] = local_out
        read_ref[u] = start_read
        near[g, u, 0, own_rows(u), :] = pack(u, transit)
        near[g, u, 1, own_rows(u), :] = pack(u, added)
    for u in range(len(units)):
        for e in range(1, T):
            near_copy(u, e).start()

    @pl.when(m == 0)
    def _():
        chain_in[...] = jnp.zeros_like(chain_in)

    open_weight(1)
    open_weight(2)

    def chain_copy(u):
        return remote(
            chain_out.at[u, own_rows(u)], chain_in.at[u, own_rows(u)], chain_sem_out.at[u], chain_sem_in.at[u],
            member(1) * T + g, t,
        )

    for u in range(len(units)):
        for e in range(1, T):
            near_take(u, e).wait_recv()
        move, add = near_state(0, u, 0), near_state(0, u, 1).astype(jnp.float32)
        for other_g in range(1, T):
            step = near_state(other_g, u, 0)
            add = mm(add, step) + near_state(other_g, u, 1).astype(jnp.float32)
            move = mm(move, step).astype(jnp.bfloat16)
        total_move[u] = move
        total_add[u] = add
    for u in range(len(units)):

        @pl.when(m > 0)
        def _():
            chain_copy(u).wait_recv()

        before = unpack(u, chain_in[u, own_rows(u), :])
        chain_out[u, own_rows(u), :] = pack(u, mm(before, total_move[u]) + total_add[u])

        @pl.when(m < F - 1)
        def _():
            chain_copy(u).start()

    send_near_first(1, True, every)
    send_near_first(2, True, first)
    relay_weight(0, range(parts))

    def fold(other_g, states):
        return tuple(
            mm(s, near_state(other_g, u, 0)) + near_state(other_g, u, 1).astype(jnp.float32)
            for u, s in enumerate(states)
        )

    states = lax.fori_loop(
        0, g, fold, tuple(
            unpack(u, chain_in[u, own_rows(u), :]).astype(jnp.float32) for u in range(len(units))
        )
    )
    for u, (group, c) in enumerate(units):
        lanes = slice(c * LANES, (c + 1) * LANES)
        read = local_ref[u] + mm_nt(read_ref[u], states[u])
        mixed_ref[:, u * LANES : (u + 1) * LANES] = finish_unit(
            widths[group], read, load(q_ref, group, c), load(k_ref, group, c),
            load(v_ref, group, c), gain_ref[group : group + 1, lanes],
            own_ref[group : group + 1, lanes], load(g_ref, group, c),
        )

    project_copy.wait()
    mixed = mixed_ref[...]

    def columns(at):
        return pl.ds(pl.multiple_of(at * own_cols, own_cols), own_cols)

    def term(at):
        return jnp.dot(mixed, project[:, columns(at)], preferred_element_type=jnp.float32)

    def pair_copy(h, l):
        return remote(
            pair_send.at[h, l], pair_got.at[h, l], pair_out.at[h, l], pair_in.at[h, l],
            me, cell(0, l),
        )

    def term_copy(h):
        return remote(
            term_send.at[h], term_got.at[h], term_out.at[h], term_in.at[h], me, cell(h, 0)
        )

    far = list(range(1, HI)) + [0]
    for h in far:
        for l in range(1, LO):
            pair_send[h, l] = term(cell(h, l)).astype(jnp.bfloat16)
            pair_copy(h, l).start()
    for h in far:
        branch = term(cell(h, 0))
        for l in range(1, LO):
            pair_copy(h, l).wait_recv()
            branch = branch + pair_got[h, l].astype(jnp.float32)
        if h:
            term_send[h] = branch.astype(jnp.bfloat16)
            term_copy(h).start()
    for h in range(1, HI):
        term_copy(h).wait_recv()
        branch = branch + term_got[h].astype(jnp.float32)

    def positions(at):
        return pl.ds(pl.multiple_of(at * tokens, tokens), tokens)

    own_state = (residual_ref[:, columns(t)].astype(jnp.float32) + branch).astype(jnp.bfloat16)
    hidden[positions(m), columns(t)] = own_state

    def block(a, at):
        return hidden.at[positions(a), columns(at)]

    def row_copy(a, d):
        return remote(
            block(a, t), block(a, t), row_out.at[d], row_in.at[a], member(d) * T + g, t
        )

    def nearer(b, a):
        return (b // 2 == a // 2) | ((a > b) == (b % 2 == 1)) | (F % 2 == 1)

    def mate_copy(a):
        return remote(
            block(a, t), block(a, t), mate_out.at[a], row_in.at[a],
            (m + 1 - 2 * (m % 2)) * T + g, t,
        )

    def hands_on(a):
        return nearer(m, a) & (a // 2 != m // 2) & (F % 2 == 0)

    def up_copy(a, h):
        return remote(block(a, t), block(a, t), up_out.at[a, h], up_in.at[a, h], me, cell(h, 0))

    def up_take(a, h):
        at = block(a, cell(-h, 0))
        return remote(at, at, up_out.at[a, h], up_in.at[a, h], me, t)

    def side_copy(a, h, l):
        at = block(a, cell(-h, 0))
        return remote(at, at, side_out.at[a, h, l], side_in.at[a, h, l], me, cell(0, l))

    def side_take(a, h, l):
        at = block(a, cell(-h, -l))
        return remote(at, at, side_out.at[a, h, l], side_in.at[a, h, l], me, t)

    def spread(a):
        for h in range(1, HI):
            up_copy(a, h).start()
        for l in range(1, LO):
            side_copy(a, 0, l).start()

    width = wide.shape[2]
    have = (base + more(m).astype(jnp.int32)) * LANES if extra else width

    def activate(a):
        state = hidden[positions(a), :].astype(jnp.float32)
        power = jnp.sum(state * state, axis=1, keepdims=True) / depth
        normed = (state * lax.rsqrt(power + norm_epsilon) * scale_ref[...]).astype(jnp.bfloat16)
        gate_pre = jnp.dot(normed, wide[0], preferred_element_type=jnp.float32)
        up_pre = jnp.dot(normed, wide[1], preferred_element_type=jnp.float32)
        value = gate_pre / (1.0 + jnp.exp(-gate_pre)) * up_pre
        if extra:
            lane = lax.broadcasted_iota(jnp.int32, (1, width), 1)
            value = jnp.where(lane < have, value, 0.0)
        active[positions(a), :] = value.astype(jnp.bfloat16)

    for d in range(1, F):
        pl.when((m + d < F) & nearer(member(d), m))(lambda: row_copy(m, d).start())
    for d in range(1, F):
        pl.when((m + d >= F) & nearer(member(d), m))(lambda: row_copy(m, d).start())
    spread(m)
    send_weight(2, True, rest)
    send_weight(2, False, rest)
    relay_weight(1, range(parts))

    def turn(k):
        return jnp.where(k == 0, m, k - 1 + (k - 1 >= m).astype(jnp.int32))

    def target(k):
        rising = k + (k >= m).astype(jnp.int32)
        falling = F - 1 - k - (F - 1 - k <= m).astype(jnp.int32)
        return jnp.where(k == F - 1, m, jnp.where(2 * m >= F, rising, falling))

    def low_copy(k, h, l):
        return remote(
            low_send.at[k, h, l], low_got.at[k, h, l], low_out.at[k, h, l],
            low_in.at[k, h, l], me, cell(0, l),
        )

    def high_copy(k, h):
        return remote(
            high_send.at[k, h], high_got.at[k, h], high_out.at[k, h], high_in.at[k, h],
            me, cell(h, 0),
        )

    def line_copy(k):
        return remote(
            line_send.at[k], line_got.at[m], line_out.at[k], line_in.at[m], target(k) * T + g, t
        )

    def line_take(a):
        return remote(line_send.at[0], line_got.at[a], line_out.at[0], line_in.at[a], me, t)

    def across(k):
        for h in range(1, HI):
            up_take(turn(k), h).wait_recv()
            for l in range(1, LO):
                side_copy(turn(k), h, l).start()

    def gathered(k):
        for h in range(HI):
            for l in range(1, LO):
                side_take(turn(k), h, l).wait_recv()
        activate(turn(k))

    def contract(k):
        here = positions(target(k))
        units_here = active[here, :]
        for s in range(n_sp):
            summed[here, s * down_cols : (s + 1) * down_cols] = jnp.dot(
                units_here, tall[s], preferred_element_type=jnp.float32
            )
        for h in far:
            for l in range(1, LO):
                low_send[k, h, l] = summed[here, columns(cell(h, l))].astype(jnp.bfloat16)
                low_copy(k, h, l).start()

    def two_cores(k, h):
        value = summed[positions(target(k)), columns(cell(h, 0))]
        for l in range(1, LO):
            value = value + low_got[k, h, l].astype(jnp.float32)
        return value

    def halve(k):
        for h in range(HI):
            for l in range(1, LO):
                low_copy(k, h, l).wait_recv()
        for h in range(1, HI):
            high_send[k, h] = two_cores(k, h).astype(jnp.bfloat16)
            high_copy(k, h).start()

    def whole(k):
        value = two_cores(k, 0)
        for h in range(1, HI):
            high_copy(k, h).wait_recv()
            value = value + high_got[k, h].astype(jnp.float32)
        return value

    across(0)

    @pl.loop(1, F + 1)
    def _(i):
        @pl.when(i < F)
        def _():
            row_copy(turn(i), 0).wait_recv()
            pl.when(hands_on(turn(i)))(lambda: mate_copy(turn(i)).start())
            spread(turn(i))

            @pl.when(i == 1)
            def _():
                relay_weight(2, first)

            @pl.when(i == F - 1)
            def _():
                relay_weight(2, rest)

        @pl.when(i >= 2)
        def _():
            across(i - 1)

        @pl.when(i == 2)
        def _():
            arrived_weight(0)
            arrived_weight(1)

        @pl.when(i >= 3)
        def _():
            gathered(i - 3)

    @pl.loop(max(F - 2, 0), F)
    def _(k):
        gathered(k)

    arrived_weight(2)

    @pl.loop(0, F)
    def _(k):
        contract(k)

    @pl.loop(0, F)
    def _(k):
        halve(k)

    @pl.loop(0, F - 1)
    def _(k):
        line_send[k] = whole(k).astype(jnp.bfloat16)
        line_copy(k).start()

    total[...] = hidden[positions(m), columns(t)].astype(jnp.float32) + whole(F - 1)

    @pl.loop(0, F)
    def _(a):
        @pl.when(a != m)
        def _():
            line_take(a).wait_recv()
            total[...] += line_got[a].astype(jnp.float32)

    out_ref[...] = total[...].astype(jnp.bfloat16)

    for w in range(3):
        for part in range(parts):
            for d in range(1, F):
                guarded(part, member(d), lambda: give(w, part, d).wait_send())

            def passed():
                for d in range(F):
                    for e in range(1, T):
                        hand(w, part, d, e).wait_send()

            guarded(part, m, passed)
    for u in range(len(units)):
        for e in range(1, T):
            near_copy(u, e).wait_send()

    @pl.when(m < F - 1)
    def _():
        for u in range(len(units)):
            chain_copy(u).wait_send()

    for h in range(HI):
        if h:
            term_copy(h).wait_send()
        for l in range(1, LO):
            pair_copy(h, l).wait_send()
    for d in range(F):
        if d:
            pl.when(nearer(member(d), m))(lambda: row_copy(m, d).wait_send())
            line_copy(d - 1).wait_send()
        pl.when(hands_on(d))(lambda: mate_copy(d).wait_send())
        for h in range(HI):
            if h:
                up_copy(d, h).wait_send()
                high_copy(d, h).wait_send()
            for l in range(1, LO):
                side_copy(d, h, l).wait_send()
                low_copy(d, h, l).wait_send()


def layer(n_sp, n_tp, q, k, v, f, a, e, g, gain, own, residual, scale, project, gate, up, down):
    tokens, channels = q.shape[1], q.shape[2]
    units = 2 * channels // LANES
    depth = residual.shape[1]
    cols = depth // n_tp
    F = members_of(n_sp)
    T = n_sp // F
    LO = 2 if n_tp % 2 == 0 else 1
    HI = n_tp // LO
    width = -(-(gate.shape[1] // LANES) // F) * LANES
    vmem = pl.BlockSpec(memory_space=pltpu.VMEM)
    hbm = pl.BlockSpec(memory_space=pl.ANY)
    bf16, f32 = jnp.bfloat16, jnp.float32
    sem = pltpu.SemaphoreType.DMA
    scratch = [
        pltpu.VMEM((units, tokens, LANES), f32),
        pltpu.VMEM((units, tokens, LANES), f32),
        pltpu.VMEM((T, units, 2, LANES, LANES), bf16),
        pltpu.VMEM((units, LANES, LANES), bf16),
        pltpu.VMEM((units, LANES, LANES), f32),
        pltpu.VMEM((units, LANES, LANES), bf16),
        pltpu.VMEM((units, LANES, LANES), bf16),
        pltpu.VMEM((tokens, units * LANES), bf16),
        pltpu.VMEM(project.shape, bf16),
        pltpu.VMEM((tokens, cols), f32),
        pltpu.VMEM((2, depth, width), bf16),
        pltpu.VMEM((n_sp, width, down.shape[1]), bf16),
        pltpu.VMEM((HI, LO, tokens, cols), bf16),
        pltpu.VMEM((HI, LO, tokens, cols), bf16),
        pltpu.VMEM((HI, tokens, cols), bf16),
        pltpu.VMEM((HI, tokens, cols), bf16),
        pltpu.VMEM((F * tokens, depth), bf16),
        pltpu.VMEM((F * tokens, width), bf16),
        pltpu.VMEM((F * tokens, depth), f32),
        pltpu.VMEM((F, HI, LO, tokens, cols), bf16),
        pltpu.VMEM((F, HI, LO, tokens, cols), bf16),
        pltpu.VMEM((F, HI, tokens, cols), bf16),
        pltpu.VMEM((F, HI, tokens, cols), bf16),
        pltpu.VMEM((F, tokens, cols), bf16),
        pltpu.VMEM((F, tokens, cols), bf16),
        sem, sem((3, 2)),
    ]
    for shape in (
        (3, 2, F), (3, 2, F, T), (units, T), (units,), (HI, LO), (HI,), (F,), (F, HI), (F, HI, LO),
        (F, HI, LO), (F, HI), (F,),
    ):
        scratch += [sem(shape), sem(shape)]
    scratch.append(sem((F,)))
    return pl.pallas_call(
        functools.partial(layer_kernel, n_sp, n_tp, (DS, DL)),
        out_shape=jax.ShapeDtypeStruct((tokens, cols), bf16),
        in_specs=[vmem] * 11 + [hbm] * 4,
        out_specs=vmem,
        scratch_shapes=scratch,
        compiler_params=pltpu.CompilerParams(
            collective_id=0, has_side_effects=True, vmem_limit_bytes=60 * 2**20
        ),
        name="layer",
    )(q, k, v, f, a, e, g, gain, own, residual, scale, project, gate, up, down)


def on_device(
    stratum_source_matrix,
    acceptance_query,
    cluster_lookup_matrix,
    cluster_payload_matrix,
    fading_logit,
    adaptation_speed_logit,
    additional_fading_exponent,
    result_switch_pair,
    attender_scaling_factor,
    present_item_factor,
    final_mapping_matrix,
    perceptron_scaling_factor,
    switching_matrix,
    widening_matrix,
    shrinking_matrix,
):
    return layer(
        lax.axis_size("sp"),
        lax.axis_size("tp"),
        acceptance_query,
        cluster_lookup_matrix,
        cluster_payload_matrix,
        fading_logit,
        adaptation_speed_logit,
        additional_fading_exponent,
        result_switch_pair,
        attender_scaling_factor,
        present_item_factor,
        stratum_source_matrix,
        perceptron_scaling_factor.reshape(1, -1),
        final_mapping_matrix.reshape(-1, final_mapping_matrix.shape[2]),
        switching_matrix,
        widening_matrix,
        shrinking_matrix,
    )


def solution(mesh):
    tokens = P(None, "sp", "tp")
    in_specs = (
        P("sp", None), tokens, tokens, tokens, tokens, tokens, tokens, tokens,
        P(None, "tp"), P(None, "tp"), P(None, "tp", None), P(),
        P("sp", "tp"), P("sp", "tp"), P("tp", "sp"),
    )
    return jax.shard_map(
        on_device, mesh=mesh, in_specs=in_specs, out_specs=P("sp", "tp"), check_vma=False
    )
```
